128 devices in a mesh: sp: 16 (over z, x), tp: 8 (over y, core).
Axes of the slice: x: 4, y: 4, z: 4, core: 2. Of those that a mesh axis runs over, the one named last changes fastest.
Arguments:
- latent: bfloat16 [2, 8192, 2048], P(None, ('sp', 'tp')), may hold values from -6 to 6
- context: bfloat16 [2, 1024, 2048], P(None, 'sp'), may hold values from -6 to 6
- cond: bfloat16 [2, 2048], replicated, may hold values from -6 to 6
- ctx_cond: bfloat16 [2048], replicated, may hold values from -6 to 6
- w_shift: bfloat16 [2048, 2048], P('sp', 'tp'), may hold values from -0.125 to 0.125
- w_scale: bfloat16 [2048, 2048], P('sp', 'tp'), may hold values from -0.125 to 0.125
- w_gate: bfloat16 [2048, 2048], P('sp', 'tp'), may hold values from -0.125 to 0.125
- norm_gain: float32 [2048], replicated, may hold values from 0.1 to 1.9
- w_query: bfloat16 [2048, 2048], P(None, 'tp'), may hold values from -1.08275726 to 1.08275726
- w_key: bfloat16 [2048, 2048], P(None, 'tp'), may hold values from -0.090598056 to 0.090598056
- w_value: bfloat16 [2048, 2048], P(None, 'tp'), may hold values from -0.125 to 0.125
- w_out: bfloat16 [2048, 2048], P('tp'), may hold values from -1.5 to 1.5
- rel_bias: float32 [32, 15, 31], P('tp'), may hold values from -4 to 4
- ctx_bias: float32 [32], P('tp'), may hold values from -3.5 to -2
Outputs:
- mixed: bfloat16 [2, 8192, 2048], P(None, ('sp', 'tp'))
The draws below stay inside these ranges and needn't reach their ends.
All inputs are finite; a program needn't handle non-finite values.
Results may differ from the reference program's by a relative error of at most 0.0154.
Values may be sent and summed in bfloat16 or wider, within the bound.
A program may use at most 128 MiB of HBM per device.

```python
import jax
import jax.numpy as jnp
from jax import lax

D = 2048
HEADS = 32
HEAD_DIM = 64
GRID_W = 64
WIN_ROWS = 8
WIN_COLS = 16
SAMPLES = 2
ROWS = 128
TOKENS = 8192
CTX = 1024
N_TP = 8


def shared_keys(key):
    base = jax.random.normal(jax.random.fold_in(key, 11), (D, D), jnp.float32)
    return jnp.clip(base, -4.0, 4.0) * D ** (-0.5)


def draw_w_key(key, part):
    return shared_keys(key).astype(jnp.bfloat16)


def draw_w_query(key, part):
    own = jax.random.normal(jax.random.fold_in(key, 12), (D, D), jnp.float32)
    own = jnp.clip(own, -4.0, 4.0) * D ** (-0.5)
    return own.astype(jnp.bfloat16)


def levels(own_key, extent, pieces, smallest, high):
    loudness, own = 1.0, jax.random.fold_in(own_key, 6)
    for axis_at, parts in pieces:
        steps = jnp.exp(jax.random.uniform(jax.random.fold_in(own, axis_at), (parts,), jnp.float32, smallest / len(pieces), high / len(pieces)))
        loudness = loudness * jnp.repeat(steps, extent[axis_at] // parts).reshape([-1 if axis == axis_at else 1 for axis in range(len(extent))])
    return loudness


def noise(stream_key, extent, width, limit, shards=(), kind=jnp.bfloat16):
    entries = jax.random.normal(stream_key, extent, jnp.float32) * width
    if len(shards) > 0:
        entries = levels(stream_key, extent, shards, -0.22, 0.18) * entries
    return jnp.clip(entries, min=-limit, max=limit).astype(kind)


def setup_inputs(seed: int = 0) -> dict:
    key_list = jax.random.split(jax.random.key(seed), 15)
    return {
        "latent": noise(key_list[0], (SAMPLES, TOKENS, D), 1.0, 6.0, ((1, 128),)),
        "context": noise(key_list[1], (SAMPLES, CTX, D), 1.0, 6.0, ((1, 16),)),
        "cond": noise(key_list[2], (SAMPLES, D), 1.0, 6.0),
        "ctx_cond": noise(key_list[3], (D,), 1.0, 6.0),
        "w_shift": noise(key_list[4], (D, D), D ** -0.5, 0.125, ((0, 16), (1, 8))),
        "w_scale": noise(key_list[5], (D, D), D ** -0.5, 0.125, ((0, 16), (1, 8))),
        "w_gate": noise(key_list[6], (D, D), D ** -0.5, 0.125, ((0, 16), (1, 8))),
        "norm_gain": jnp.clip(1.0 + 0.18 * jax.random.normal(key_list[7], (D,), jnp.float32), 0.1, 1.9),
        "w_query": draw_w_query(jax.random.fold_in(key_list[14], 71), 0),
        "w_key": draw_w_key(jax.random.fold_in(key_list[14], 71), 0),
        "w_value": noise(key_list[10], (D, D), D ** -0.5, 0.125, ((1, 8),)),
        "w_out": noise(key_list[11], (D, D), 16 ** -0.5, 1.5, ((0, 8),)),
        "rel_bias": noise(key_list[12], (HEADS, 2 * WIN_ROWS - 1, 2 * WIN_COLS - 1), 1.0, 4.0, ((0, 8),), jnp.float32),
        "ctx_bias": jnp.clip(-3.5 + 1.5 * jax.random.uniform(key_list[13], (HEADS,), jnp.float32) ** levels(key_list[13], (HEADS,), ((0, 8),), -0.2, 0.2), -3.5, -2.0),
    }


EPSILON = 1e-06

def modulate_rows(rows, gain, shift, scale):
    floats = rows.astype(jnp.float32)
    inverse = lax.rsqrt(lax.optimization_barrier(jnp.mean(floats * floats, axis=-1, keepdims=True)) + EPSILON)
    return (floats * inverse * gain * (1.0 + scale) + shift).astype(jnp.bfloat16)

def project(rows, weight):
    return jnp.dot(rows, weight, preferred_element_type=jnp.float32).astype(jnp.bfloat16)

def reference(latent, context, cond, ctx_cond, w_shift, w_scale, w_gate, norm_gain, w_query, w_key, w_value, w_out, rel_bias, ctx_bias):
    ada = jax.nn.silu(cond.astype(jnp.float32)).astype(jnp.bfloat16)
    ada_ctx = jax.nn.silu(ctx_cond.astype(jnp.float32)).astype(jnp.bfloat16)[None, :]
    shift = jnp.dot(ada, w_shift, preferred_element_type=jnp.float32)
    scale = jnp.dot(ada, w_scale, preferred_element_type=jnp.float32)
    gate = jnp.dot(ada, w_gate, preferred_element_type=jnp.float32)
    ctx_shift = jnp.dot(ada_ctx, w_shift, preferred_element_type=jnp.float32)[0]
    ctx_scale = jnp.dot(ada_ctx, w_scale, preferred_element_type=jnp.float32)[0]
    hidden = modulate_rows(latent, norm_gain, shift[:, None, :], scale[:, None, :])
    ctx_hidden = modulate_rows(context, norm_gain, ctx_shift, ctx_scale)
    query = project(hidden, w_query).reshape(SAMPLES, ROWS, GRID_W, HEADS, HEAD_DIM)
    key = project(hidden, w_key).reshape(SAMPLES, ROWS, GRID_W, HEADS, HEAD_DIM)
    value = project(hidden, w_value).reshape(SAMPLES, ROWS, GRID_W, HEADS, HEAD_DIM)
    ctx_key = project(ctx_hidden, w_key).reshape(SAMPLES, CTX, HEADS, HEAD_DIM).astype(jnp.float32)
    ctx_value = project(ctx_hidden, w_value).reshape(SAMPLES, CTX, HEADS, HEAD_DIM).astype(jnp.float32)
    factor = HEAD_DIM ** (-0.5)
    columns = jnp.arange(GRID_W, dtype=jnp.int32)
    col_start = jnp.clip(columns - WIN_COLS // 2, 0, GRID_W - WIN_COLS)
    col_mask = (columns[None, :] >= col_start[:, None]) & (columns[None, :] < col_start[:, None] + WIN_COLS)
    col_index = jnp.clip(columns[None, :] - columns[:, None] + WIN_COLS - 1, 0, 2 * WIN_COLS - 2)

    def one_row(row):
        first = jnp.clip(row - WIN_ROWS // 2, 0, ROWS - WIN_ROWS).astype(jnp.int32)
        query_row = lax.dynamic_index_in_dim(query, row, axis=1, keepdims=False).astype(jnp.float32)
        key_rows = lax.dynamic_slice_in_dim(key, first, WIN_ROWS, axis=1).astype(jnp.float32)
        value_rows = lax.dynamic_slice_in_dim(value, first, WIN_ROWS, axis=1).astype(jnp.float32)
        row_index = first + jnp.arange(WIN_ROWS, dtype=jnp.int32) - row + WIN_ROWS - 1
        bias = rel_bias[:, row_index][:, :, col_index]
        near = jnp.einsum('sqhd,siwhd->shqiw', query_row, key_rows) * factor + bias.transpose(0, 2, 1, 3)[None]
        near = jnp.where(col_mask[None, None, :, None, :], near, -jnp.inf).reshape(SAMPLES, HEADS, GRID_W, WIN_ROWS * GRID_W)
        far = jnp.einsum('sqhd,schd->shqc', query_row, ctx_key) * factor + ctx_bias[None, :, None, None]
        top = jnp.maximum(lax.optimization_barrier(jnp.max(near, axis=-1)), lax.optimization_barrier(jnp.max(far, axis=-1)))[..., None]
        near_exp = jnp.exp(near - top)
        far_exp = jnp.exp(far - top)
        total = lax.optimization_barrier(jnp.sum(near_exp, axis=-1, keepdims=True)) + lax.optimization_barrier(jnp.sum(far_exp, axis=-1, keepdims=True))
        near_weight = (near_exp / total).astype(jnp.bfloat16).astype(jnp.float32)
        far_weight = (far_exp / total).astype(jnp.bfloat16).astype(jnp.float32)
        near_weight = near_weight.reshape(SAMPLES, HEADS, GRID_W, WIN_ROWS, GRID_W)
        mixed = jnp.einsum('shqiw,siwhd->sqhd', near_weight, value_rows) + jnp.einsum('shqc,schd->sqhd', far_weight, ctx_value)
        return mixed.astype(jnp.bfloat16)
    attended = lax.map(one_row, jnp.arange(ROWS, dtype=jnp.int32))
    attended = attended.transpose(1, 0, 2, 3, 4).reshape(SAMPLES, TOKENS, D)
    group = D // N_TP
    update = jnp.zeros((SAMPLES, TOKENS, D), jnp.float32)
    for index in range(N_TP):
        part = jnp.dot(attended[..., index * group:(index + 1) * group], w_out[index * group:(index + 1) * group], preferred_element_type=jnp.float32).astype(jnp.bfloat16)
        part = lax.optimization_barrier(part)
        update = update + part.astype(jnp.float32)
    mixed_out = latent.astype(jnp.float32) + gate[:, None, :] * update
    return mixed_out.astype(jnp.bfloat16)
```

```python
import functools

import jax
import jax.numpy as jnp
from jax import lax
from jax.experimental import pallas as pl
from jax.experimental.pallas import tpu as pltpu
from jax.sharding import PartitionSpec as P

MESH = pl.DeviceIdType.MESH
F32, BF16 = jnp.float32, jnp.bfloat16
N_SP, N_TP, NX, NZ, NY = 16, 8, 4, 4, 4
D = 2048
W = 64
EPSILON = 1e-06
LOG2E = 1.4426950408889634
MASKED = -1e30


def silu(v):
    return v / (1.0 + jnp.exp(-v))


def modulated(x, gain, shift):
    f = x.astype(F32)
    inv = lax.rsqrt(jnp.mean(f * f, axis=-1, keepdims=True) + EPSILON)
    return (f * inv * gain + shift).astype(BF16)


def remote(src, dst, send, recv, sp, tp):
    return pltpu.make_async_remote_copy(
        src_ref=src, dst_ref=dst, send_sem=send, recv_sem=recv, device_id=(sp, tp), device_id_type=MESH
    )


def front_kernel(
    latent, context, cond, ctx_cond, wsh, wsc, wga, gain, wq, wk, wv, wo, relb,
    q_out, kv_out, ckv_out, wo_out, rel_out, gate_out,
    lat, ctx, wmod, wbuf, ada, modrecv, modall, hid,
    loc_sem, w_send, w_recv, lat_send, lat_recv, m1_send, m1_recv, m2_send, m2_recv,
    ca_send, ca_recv, cb_send, cb_recv, h_send, h_recv,
):
    sp, tp = lax.axis_index("sp"), lax.axis_index("tp")
    y, c = tp // 2, tp % 2
    z, x = sp // 4, sp % 4
    o = 1 - c
    up, down, opp = (y + 1) % 4, (y + 3) % 4, (y + 2) % 4

    barrier = pltpu.get_barrier_semaphore()
    for d in range(1, N_SP):
        pl.semaphore_signal(barrier, inc=1, device_id=((sp + d) % N_SP, tp), device_id_type=MESH)
    for d in range(1, N_TP):
        pl.semaphore_signal(barrier, inc=1, device_id=(sp, (tp + d) % N_TP), device_id_type=MESH)

    local = [
        pltpu.make_async_copy(wsh, wmod.at[0], loc_sem.at[0]),
        pltpu.make_async_copy(wsc, wmod.at[1], loc_sem.at[1]),
        pltpu.make_async_copy(wga, wmod.at[2], loc_sem.at[2]),
        pltpu.make_async_copy(context.at[c], ctx, loc_sem.at[3]),
        pltpu.make_async_copy(latent.at[c], lat.at[tp], loc_sem.at[4]),
        pltpu.make_async_copy(wk, wbuf.at[c, 1], loc_sem.at[5]),
        pltpu.make_async_copy(wv, wbuf.at[c, 2], loc_sem.at[6]),
        pltpu.make_async_copy(wq, wbuf.at[c, 0], loc_sem.at[7]),
        pltpu.make_async_copy(wo, wo_out.at[c], loc_sem.at[8]),
        pltpu.make_async_copy(relb, rel_out.at[c], loc_sem.at[9]),
    ]
    for cp in local:
        cp.start()
    pl.semaphore_wait(barrier, N_SP + N_TP - 2)

    def lat_copy(s, k, yy, j, slot):
        return remote(latent.at[s], lat.at[tp], lat_send.at[k], lat_recv.at[slot], sp, 2 * yy + j)

    lats = [
        lat_copy(c, 0, up, c, 1 + c),
        lat_copy(c, 1, down, c, 3 + c),
        lat_copy(o, 2, up, o, 1 + c),
        lat_copy(o, 3, down, o, 3 + c),
        lat_copy(o, 4, y, o, 0),
    ]
    pair = tp + 1 - 2 * c
    weights = [
        remote(wk, wbuf.at[c, 1], w_send.at[0], w_recv.at[0], sp, pair),
        remote(wv, wbuf.at[c, 2], w_send.at[1], w_recv.at[1], sp, pair),
        remote(wq, wbuf.at[c, 0], w_send.at[2], w_recv.at[2], sp, pair),
        remote(wo, wo_out.at[c], w_send.at[3], w_recv.at[3], sp, pair),
        remote(relb, rel_out.at[c], w_send.at[4], w_recv.at[4], sp, pair),
    ]
    for cp in lats + weights:
        cp.start()

    at = pl.ds(pl.multiple_of(sp * 128, 128), 128)
    ada[...] = jnp.zeros_like(ada)
    ada[0:2] = silu(cond[:, at].astype(F32))
    ada[2:3] = silu(ctx_cond[:, at].astype(F32))
    rows = ada[...].astype(BF16)
    for cp in local[:3]:
        cp.wait()
    sums = [jnp.dot(rows, wmod[i], preferred_element_type=F32) for i in range(3)]
    modrecv[0, 0:3] = sums[0][0:3]
    modrecv[0, 3:6] = sums[1][0:3]
    modrecv[0, 6:8] = sums[2][0:2]
    m1 = [
        remote(modrecv.at[0], modrecv.at[d], m1_send.at[d], m1_recv.at[d], (sp + d) % N_SP, tp)
        for d in range(1, N_SP)
    ]
    for cp in m1:
        cp.start()
    for cp in m1:
        cp.wait_recv()
    modall[tp] = jnp.sum(modrecv[...], axis=0)
    m2 = [
        remote(modall.at[tp], modall.at[tp], m2_send.at[d], m2_recv.at[d], sp, (tp + d) % N_TP)
        for d in range(1, N_TP)
    ]
    for cp in m2:
        cp.start()
    for d in range(1, N_TP):
        mine = modall.at[(tp + N_TP - d) % N_TP]
        remote(mine, mine, m2_send.at[d], m2_recv.at[d], sp, (tp + d) % N_TP).wait_recv()

    def mod_row(i):
        return jnp.concatenate([modall[t, pl.ds(i, 1), :] for t in range(N_TP)], axis=1)

    g = gain[...]
    for s in range(2):
        gate_out[s : s + 1] = mod_row(6 + s)
    shift, scaled = mod_row(c), g * (1.0 + mod_row(3 + c))
    ctx_shift, ctx_scaled = mod_row(2), g * (1.0 + mod_row(5))

    for cp in local[3:8]:
        cp.wait()
    hid[0:64] = modulated(ctx[...], ctx_scaled, ctx_shift)
    theirs = [
        remote(wk, wbuf.at[o, 1], w_send.at[0], w_recv.at[0], sp, pair),
        remote(wv, wbuf.at[o, 2], w_send.at[1], w_recv.at[1], sp, pair),
        remote(wq, wbuf.at[o, 0], w_send.at[2], w_recv.at[2], sp, pair),
        remote(wo, wo_out.at[o], w_send.at[3], w_recv.at[3], sp, pair),
        remote(relb, rel_out.at[o], w_send.at[4], w_recv.at[4], sp, pair),
    ]
    for cp in theirs[:3]:
        cp.wait_recv()
    for j in range(2):
        for kind in range(2):
            ckv_out[kind, z, x, :, 256 * j : 256 * (j + 1)] = jnp.dot(
                hid[0:64], wbuf[j, 1 + kind], preferred_element_type=F32
            ).astype(BF16)
    first = []
    for d in range(1, 4):
        own = ckv_out.at[0, z, x]
        first.append(
            remote(own, own, ca_send.at[d - 1], ca_recv.at[d - 1], 4 * z + (x + d) % 4, tp)
        )
        own = ckv_out.at[1, z, x]
        first.append(
            remote(own, own, ca_send.at[d + 2], ca_recv.at[d + 2], 4 * ((z + d) % 4) + x, tp)
        )
    for cp in first:
        cp.start()

    def unit(yy, k):
        for r in range(2):
            hid[64 * r : 64 * (r + 1)] = modulated(lat[2 * yy + r], scaled, shift)
        rows_q = pl.ds(pl.multiple_of(yy * 128, 128), 128)
        rows_k = pl.ds(pl.multiple_of(256 + yy * 128, 128), 128)
        for kind in (1, 2, 0):
            for j in range(2):
                cols = slice(256 * j, 256 * (j + 1))
                r = jnp.dot(hid[...], wbuf[j, kind], preferred_element_type=F32)
                if kind == 0:
                    q_out[rows_q, cols] = (r * (0.125 * LOG2E)).astype(BF16)
                else:
                    kv_out[kind - 1, rows_k, cols] = r.astype(BF16)
        hi = yy // 2
        to = pl.multiple_of(128 * (yy - 2 * hi) + 768 * (1 - hi), 128)
        cp = remote(
            kv_out.at[:, rows_k, :],
            kv_out.at[:, pl.ds(to, 128), :],
            h_send.at[k],
            h_recv.at[yy],
            (sp + 2 * hi - 1 + N_SP) % N_SP,
            tp,
        )
        cp.start()
        return cp

    def lat_wait(row, slot):
        ref = lat.at[row]
        remote(ref, ref, lat_send.at[slot], lat_recv.at[slot], sp, pair).wait_recv()

    lat_wait(2 * y + o, 0)
    halos = [unit(y, 0)]

    lat_wait(2 * down, 1)
    ref = lat.at[2 * down]
    lats.append(remote(ref, ref, lat_send.at[5], lat_recv.at[5], sp, 2 * up + c))
    lats[-1].start()
    lat_wait(2 * up + 1, 4)
    ref = lat.at[2 * up + 1]
    lats.append(remote(ref, ref, lat_send.at[6], lat_recv.at[6], sp, 2 * down + c))
    lats[-1].start()

    for d in range(1, 4):
        ref = ckv_out.at[0, z, (x + 4 - d) % 4]
        remote(ref, ref, ca_send.at[d - 1], ca_recv.at[d - 1], sp, pair).wait_recv()
        ref = ckv_out.at[1, (z + 4 - d) % 4, x]
        remote(ref, ref, ca_send.at[d + 2], ca_recv.at[d + 2], sp, pair).wait_recv()
    second = []
    for d in range(1, 4):
        ref = ckv_out.at[0, z]
        second.append(
            remote(ref, ref, cb_send.at[d - 1], cb_recv.at[d - 1], 4 * ((z + d) % 4) + x, tp)
        )
        ref = ckv_out.at[1, :, x]
        second.append(
            remote(ref, ref, cb_send.at[d + 2], cb_recv.at[d + 2], 4 * z + (x + d) % 4, tp)
        )
    for cp in second:
        cp.start()

    lat_wait(2 * down + 1, 2)
    halos.append(unit(down, 1))
    lat_wait(2 * up, 3)
    halos.append(unit(up, 2))
    lat_wait(2 * opp, 5)
    lat_wait(2 * opp + 1, 6)
    halos.append(unit(opp, 3))

    for d in range(1, 4):
        ref = ckv_out.at[0, (z + 4 - d) % 4]
        remote(ref, ref, cb_send.at[d - 1], cb_recv.at[d - 1], sp, pair).wait_recv()
        ref = ckv_out.at[1, :, (x + 4 - d) % 4]
        remote(ref, ref, cb_send.at[d + 2], cb_recv.at[d + 2], sp, pair).wait_recv()
    for yy in range(4):
        hi = yy // 2
        ref = kv_out.at[:, pl.ds(128 * (yy - 2 * hi) + 768 * (1 - hi), 128), :]
        remote(ref, ref, h_send.at[yy], h_recv.at[yy], sp, pair).wait_recv()
    for cp in theirs[3:]:
        cp.wait_recv()
    for cp in local[8:]:
        cp.wait()
    for cp in lats + weights + m1 + m2 + first + second + halos:
        cp.wait_send()


def attention_kernel(q, kv, ckv, wo, rel, part, table, far_o, far_m, att):
    sp = lax.axis_index("sp")
    lane = lax.broadcasted_iota(jnp.int32, (W, 128), 1)
    col = lax.broadcasted_iota(jnp.int32, (W, 128), 0)
    key = lane % W
    start = jnp.clip(col - 8, 0, 48)
    inside = (key >= start) & (key < start + 16)

    def build(h, _):
        def one(a, carry):
            r0 = jnp.broadcast_to(rel[h, pl.ds(a, 1), :], (W, 128))
            r1 = jnp.broadcast_to(rel[h, pl.ds(a + 1, 1), :], (W, 128))
            r0 = pltpu.roll(r0, 113, 1, stride=1, stride_axis=0)
            r1 = pltpu.roll(r1, 113 - 64, 1, stride=1, stride_axis=0)
            table[h, a] = jnp.where(inside, jnp.where(lane < W, r0, r1) * LOG2E, MASKED)
            return carry

        return lax.fori_loop(0, 14, one, 0)

    lax.fori_loop(0, 8, build, 0)
    ones_far = jnp.ones((1024, 128), BF16)
    ones_near = jnp.ones((512, 128), BF16)

    for hp in range(4):
        lanes = slice(128 * hp, 128 * (hp + 1))
        qp, kp = q[:, lanes], ckv[0, :, lanes]
        vp = jnp.concatenate([ckv[1, :, lanes], ones_far], axis=1)
        first = lax.broadcasted_iota(jnp.int32, (512, 128), 1) < W
        for half in range(2):
            h = 2 * hp + half
            qh = jnp.where(first if half == 0 else ~first, qp, jnp.zeros_like(qp))
            s = lax.dot_general(qh, kp, (((1,), (1,)), ((), ())), preferred_element_type=F32)
            m = jnp.max(s, axis=-1, keepdims=True)
            p = jnp.exp2(s - m).astype(BF16)
            far_o[h] = jnp.dot(p, vp, preferred_element_type=F32)
            far_m[h] = m + rel[h, 15:16, :] * LOG2E

    def rows_two(i, carry):
        for r in range(2):
            row = 2 * i + r
            g = sp * 8 + row
            r0 = jnp.clip(g - 4, 0, 120)
            base = pl.multiple_of((r0 - sp * 8 + 4) * W, W)
            a0 = r0 - g + 7
            at = pl.ds(pl.multiple_of(row * W, W), W)
            for hp in range(4):
                lanes = slice(128 * hp, 128 * (hp + 1))
                qp = q[at, lanes]
                kp = kv[0, pl.ds(base, 512), lanes]
                vp = jnp.concatenate([kv[1, pl.ds(base, 512), lanes], ones_near], axis=1)
                outs = []
                for half in range(2):
                    h = 2 * hp + half
                    mine = lane < W if half == 0 else lane >= W
                    qh = jnp.where(mine, qp, jnp.zeros_like(qp))
                    s = lax.dot_general(qh, kp, (((1,), (1,)), ((), ())), preferred_element_type=F32)
                    s = s + jnp.concatenate([table[h, a0 + 2 * k] for k in range(4)], axis=1)
                    m1 = far_m[h, at, :]
                    m = jnp.maximum(jnp.max(s, axis=-1, keepdims=True), m1)
                    alpha = jnp.exp2(m1 - m)
                    p = jnp.exp2(s - jnp.concatenate([m] * 4, axis=1)).astype(BF16)
                    near = jnp.dot(p, vp, preferred_element_type=F32)
                    o = near[:, :128] + alpha * far_o[h, at, :128]
                    t = near[:, 128:] + alpha * far_o[h, at, 128:]
                    outs.append(o / t)
                att[W * r : W * (r + 1), lanes] = jnp.where(lane < W, outs[0], outs[1]).astype(BF16)
        part[i] = jnp.dot(att[...], wo[...], preferred_element_type=F32).astype(BF16)
        return carry

    lax.fori_loop(0, 4, rows_two, 0)


def back_kernel(part, latent, gate, out, relay, comb, inbox, r_send, r_recv, i_send, i_recv):
    sp, tp = lax.axis_index("sp"), lax.axis_index("tp")
    y, c = tp // 2, tp % 2
    o = 1 - c
    up, down, opp = (y + 1) % 4, (y + 3) % 4, (y + 2) % 4
    pair = tp + 1 - 2 * c
    barrier = pltpu.get_barrier_semaphore()
    peers = [pair, 2 * up, 2 * up + 1, 2 * down, 2 * down + 1]
    for peer in peers:
        pl.semaphore_signal(barrier, inc=1, device_id=(sp, peer), device_id_type=MESH)
    pl.semaphore_wait(barrier, len(peers))

    def row(yy, r):
        return part.at[yy, pl.ds(pl.multiple_of(r * W, W), W), :]

    relays = [
        remote(row(opp, 0), relay.at[0], r_send.at[0], r_recv.at[0], sp, 2 * up + c),
        remote(row(opp, 1), relay.at[1], r_send.at[1], r_recv.at[1], sp, 2 * down + c),
    ]
    sends = [
        remote(row(up, 1), inbox.at[c, 0], i_send.at[0], i_recv.at[c, 0], sp, 2 * up + 1),
        remote(row(down, 0), inbox.at[c, 1], i_send.at[1], i_recv.at[c, 1], sp, 2 * down),
        remote(row(y, o), inbox.at[c, 2], i_send.at[2], i_recv.at[c, 2], sp, pair),
    ]
    for cp in relays + sends:
        cp.start()
    inbox[c, 2] = part[y, pl.ds(pl.multiple_of(c * W, W), W), :]
    relays[0].wait_recv()
    comb[0] = (part[up, 0:W, :].astype(F32) + relay[0].astype(F32)).astype(BF16)
    sends.append(remote(comb.at[0], inbox.at[c, 0], i_send.at[3], i_recv.at[c, 0], sp, 2 * up))
    sends[-1].start()
    relays[1].wait_recv()
    comb[1] = (part[down, W : 2 * W, :].astype(F32) + relay[1].astype(F32)).astype(BF16)
    sends.append(
        remote(comb.at[1], inbox.at[c, 1], i_send.at[4], i_recv.at[c, 1], sp, 2 * down + 1)
    )
    sends[-1].start()

    def got(s, k):
        ref = inbox.at[s, k]
        remote(ref, ref, i_send.at[k], i_recv.at[s, k], sp, pair).wait_recv()

    got(o, 2)
    for s in range(2):
        got(s, 0)
        got(s, 1)
    for s in range(2):
        update = inbox[s, 0].astype(F32) + inbox[s, 1].astype(F32) + inbox[s, 2].astype(F32)
        out[s] = (latent[s].astype(F32) + gate[s : s + 1] * update).astype(BF16)
    for cp in relays + sends:
        cp.wait_send()


VM = pl.BlockSpec(memory_space=pltpu.VMEM)
ANY = pl.BlockSpec(memory_space=pl.ANY)
DMA = pltpu.SemaphoreType.DMA


def shape(*dims, kind=BF16):
    return jax.ShapeDtypeStruct(dims, kind)


def on_device(
    latent, context, cond, ctx_cond, w_shift, w_scale, w_gate, norm_gain,
    w_query, w_key, w_value, w_out, rel_bias, ctx_bias,
):
    relb = jnp.concatenate(
        [
            jnp.pad(rel_bias, ((0, 0), (0, 0), (0, 97))),
            jnp.broadcast_to(ctx_bias[:, None, None], (4, 1, 128)),
        ],
        axis=1,
    )
    q, kv, ckv, wo, rel, gate = pl.pallas_call(
        front_kernel,
        out_shape=[
            shape(512, 512),
            shape(2, 1024, 512),
            shape(2, NZ, NX, 64, 512),
            shape(2, 256, D),
            shape(2, 4, 16, 128, kind=F32),
            shape(2, D, kind=F32),
        ],
        in_specs=[ANY, ANY, VM, VM, ANY, ANY, ANY, VM, ANY, ANY, ANY, ANY, ANY],
        out_specs=[VM] * 6,
        scratch_shapes=[
            pltpu.VMEM((8, W, D), BF16),
            pltpu.VMEM((W, D), BF16),
            pltpu.VMEM((3, 128, 256), BF16),
            pltpu.VMEM((2, 3, D, 256), BF16),
            pltpu.VMEM((8, 128), F32),
            pltpu.VMEM((16, 8, 256), F32),
            pltpu.VMEM((8, 8, 256), F32),
            pltpu.VMEM((128, D), BF16),
            DMA((10,)),
            DMA((5,)), DMA((5,)), DMA((7,)), DMA((7,)),
            DMA((16,)), DMA((16,)), DMA((8,)), DMA((8,)),
            DMA((6,)), DMA((6,)), DMA((6,)), DMA((6,)), DMA((4,)), DMA((4,)),
        ],
        compiler_params=pltpu.CompilerParams(
            collective_id=0, has_side_effects=True, vmem_limit_bytes=40 * 2**20
        ),
        name="front",
    )(
        latent, context, cond, ctx_cond[None, :], w_shift, w_scale, w_gate, norm_gain[None, :],
        w_query, w_key, w_value, w_out, relb,
    )
    part = pl.pallas_call(
        attention_kernel,
        out_shape=shape(4, 128, D),
        in_specs=[VM] * 5,
        out_specs=VM,
        scratch_shapes=[
            pltpu.VMEM((8, 14, W, 128), F32),
            pltpu.VMEM((8, 512, 256), F32),
            pltpu.VMEM((8, 512, 128), F32),
            pltpu.VMEM((128, 512), BF16),
        ],
        compiler_params=pltpu.CompilerParams(vmem_limit_bytes=40 * 2**20),
        name="attend",
    )(q, kv, ckv.reshape(2, 1024, 512), wo.reshape(512, D), rel.reshape(8, 16, 128))
    return pl.pallas_call(
        back_kernel,
        out_shape=shape(2, W, D),
        in_specs=[VM] * 3,
        out_specs=VM,
        scratch_shapes=[
            pltpu.VMEM((2, W, D), BF16),
            pltpu.VMEM((2, W, D), BF16),
            pltpu.VMEM((2, 3, W, D), BF16),
            DMA((2,)), DMA((2,)), DMA((5,)), DMA((2, 3)),
        ],
        compiler_params=pltpu.CompilerParams(
            collective_id=1, has_side_effects=True, vmem_limit_bytes=40 * 2**20
        ),
        name="back",
    )(part, latent, gate)


def solution(mesh):
    return jax.shard_map(
        on_device,
        mesh=mesh,
        in_specs=(
            P(None, ("sp", "tp"), None),
            P(None, "sp", None),
            P(),
            P(),
            P("sp", "tp"),
            P("sp", "tp"),
            P("sp", "tp"),
            P(),
            P(None, "tp"),
            P(None, "tp"),
            P(None, "tp"),
            P("tp", None),
            P("tp", None, None),
            P("tp"),
        ),
        out_specs=P(None, ("sp", "tp"), None),
        check_vma=False,
    )
```

```python
import functools

import jax
import jax.numpy as jnp
from jax import lax
from jax.experimental import pallas as pl
from jax.experimental.pallas import tpu as pltpu
from jax.sharding import PartitionSpec as P

MESH = pl.DeviceIdType.MESH
F32, BF16 = jnp.float32, jnp.bfloat16
N_SP, N_TP, NX, NZ, NY = 16, 8, 4, 4, 4
D = 2048
W = 64
EPSILON = 1e-06
LOG2E = 1.4426950408889634
MASKED = -1e30


def silu(v):
    return v / (1.0 + jnp.exp(-v))


def modulated(x, gain, shift):
    f = x.astype(F32)
    inv = lax.rsqrt(jnp.mean(f * f, axis=-1, keepdims=True) + EPSILON)
    return (f * inv * gain + shift).astype(BF16)


def remote(src, dst, send, recv, sp, tp):
    return pltpu.make_async_remote_copy(
        src_ref=src, dst_ref=dst, send_sem=send, recv_sem=recv, device_id=(sp, tp), device_id_type=MESH
    )


def kernel(
    latent, context, cond, ctx_cond, wsh, wsc, wga, gain, wq, wk, wv, wo, rel_bias, ctx_bias,
    out,
    q, kv, ckv, wout, rel, gate, lat, ctx, wmod, wbuf, ada, ctx_ada, modrecv, modall, hid,
    table, far_o, far_m, att, part, relay, comb, inbox, mine, hlat,
    loc_sem, w_send, w_recv, lat_send, lat_recv, m1_send, m1_recv, m2_send, m2_recv,
    ca_send, ca_recv, cb_send, cb_recv, h_send, h_recv, r_send, r_recv, i_send, i_recv, raw_send, raw_recv,
):
    sp, tp = lax.axis_index("sp"), lax.axis_index("tp")
    y, c = tp // 2, tp % 2
    z, x = sp // 4, sp % 4
    o = 1 - c
    pair = tp + 1 - 2 * c
    up, down, opp = (y + 1) % 4, (y + 3) % 4, (y + 2) % 4
    z_up, z_down, x_up, x_down = (z + 1) % 4, (z + 3) % 4, (x + 1) % 4, (x + 3) % 4

    barrier = pltpu.get_barrier_semaphore()
    for d in range(1, N_SP):
        pl.semaphore_signal(barrier, inc=1, device_id=((sp + d) % N_SP, tp), device_id_type=MESH)
    for d in range(1, N_TP):
        pl.semaphore_signal(barrier, inc=1, device_id=(sp, (tp + d) % N_TP), device_id_type=MESH)

    for d in (1, N_SP - 1):
        pl.semaphore_signal(barrier, inc=1, device_id=((sp + d) % N_SP, pair), device_id_type=MESH)

    local = [
        pltpu.make_async_copy(wsh, wmod.at[0], loc_sem.at[0]),
        pltpu.make_async_copy(wsc, wmod.at[1], loc_sem.at[1]),
        pltpu.make_async_copy(wga, wmod.at[2], loc_sem.at[2]),
        pltpu.make_async_copy(context.at[c], ctx, loc_sem.at[3]),
        pltpu.make_async_copy(latent.at[c], lat.at[tp], loc_sem.at[4]),
        pltpu.make_async_copy(wk, wbuf.at[c, 1], loc_sem.at[5]),
        pltpu.make_async_copy(wv, wbuf.at[c, 2], loc_sem.at[6]),
        pltpu.make_async_copy(wq, wbuf.at[c, 0], loc_sem.at[7]),
        pltpu.make_async_copy(wo, wout.at[c], loc_sem.at[8]),
        pltpu.make_async_copy(latent, mine, loc_sem.at[9]),
    ]
    for cp in local:
        cp.start()
    rel[c] = jnp.zeros((16, 4, 128), F32)
    rel[c, 0:14, :, 0:31] = rel_bias[0:14]
    rel[c, 0:14, :, 64:95] = rel_bias[1:15]
    for h in range(4):
        rel[c, 15, h : h + 1, :] = jnp.full((1, 128), ctx_bias[h], F32)

    at = pl.ds(pl.multiple_of(sp * 128, 128), 128)
    ada[...] = jnp.zeros_like(ada)
    ada[0:2] = silu(cond[:, at].astype(F32))
    ctx_ada[...] = silu(ctx_cond[...].astype(F32)).reshape(1, D)
    ada[2:3] = ctx_ada[:, at]
    rows = ada[...].astype(BF16)
    for cp in local[:3]:
        cp.wait()
    sums = [jnp.dot(rows, wmod[i], preferred_element_type=F32) for i in range(3)]
    modrecv[0, 0:3] = sums[0][0:3]
    modrecv[0, 3:6] = sums[1][0:3]
    modrecv[0, 6:8] = sums[2][0:2]

    pl.semaphore_wait(barrier, N_SP + N_TP)

    far_first = sorted(range(1, N_SP), key=lambda d: -(min(d % 4, 4 - d % 4) + min(d // 4, 4 - d // 4)))
    m1 = [
        remote(
            modrecv.at[0],
            modrecv.at[d],
            m1_send.at[d],
            m1_recv.at[d],
            4 * ((z + d // 4) % 4) + (x + d % 4) % 4,
            tp,
        )
        for d in far_first
    ]

    def lat_copy(s, k, yy, j, slot):
        return remote(latent.at[s], lat.at[tp], lat_send.at[k], lat_recv.at[slot], sp, 2 * yy + j)

    ahead, behind = (y + 1 + 2 * c) % 4, (y + 3 + 2 * c) % 4
    lats = [
        lat_copy(o, 4, y, o, 0),
        lat_copy(c, 0, ahead, c, 1 + 3 * c),
        lat_copy(o, 2, ahead, o, 1 + 3 * c),
        lat_copy(c, 1, behind, c, 3 - c),
        lat_copy(o, 3, behind, o, 3 - c),
    ]

    own_hi = y // 2
    raw_to, raw_from = sp + 2 * own_hi - 1, sp + 1 - 2 * own_hi
    raw_out = (raw_to >= 0) & (raw_to < N_SP)
    raw_in = (raw_from >= 0) & (raw_from < N_SP)
    raws = [
        remote(latent.at[s], hlat.at[c], raw_send.at[k], raw_recv.at[c], (raw_to + N_SP) % N_SP, 2 * y + s)
        for k, s in enumerate((c, o))
    ]

    def weight_copies(j):
        pairs = [
            (rel.at[j], rel.at[j]),
            (wk if j is c else wbuf.at[j, 1], wbuf.at[j, 1]),
            (wv if j is c else wbuf.at[j, 2], wbuf.at[j, 2]),
            (wq if j is c else wbuf.at[j, 0], wbuf.at[j, 0]),
            (wo if j is c else wout.at[j], wout.at[j]),
        ]
        return [
            remote(a, b, w_send.at[i], w_recv.at[i], sp, pair) for i, (a, b) in enumerate(pairs)
        ]

    weights, theirs = weight_copies(c), weight_copies(o)
    for cp in m1 + weights[:1] + lats[:2]:
        cp.start()

    @pl.when(raw_out)
    def _():
        for cp in raws:
            cp.start()

    for cp in weights[1:]:
        cp.start()

    lane = lax.broadcasted_iota(jnp.int32, (W, 128), 1)
    col = lax.broadcasted_iota(jnp.int32, (W, 128), 0)
    key = lane % W
    start = jnp.clip(col - 8, 0, 48)
    inside = (key >= start) & (key < start + 16)

    def build(j, first, last):
        def one(h, carry):
            for a in range(14):
                r = jnp.broadcast_to(rel[j, a, pl.ds(h, 1), :] * LOG2E, (W, 128))
                r = pltpu.roll(r, 113, 1, stride=1, stride_axis=0)
                table[4 * j + h, a] = jnp.where(inside, r, MASKED)
            return carry

        lax.fori_loop(first, last, one, 0)

    build(c, 0, 4)

    for cp in m1:
        cp.wait_recv()
    modall[tp] = jnp.sum(modrecv[...], axis=0)
    m2 = [
        remote(modall.at[tp], modall.at[tp], m2_send.at[d], m2_recv.at[d], sp, (tp + d) % N_TP)
        for d in (4, 3, 5, 2, 6, 1, 7)
    ]
    for cp in m2 + lats[2:]:
        cp.start()
    theirs[0].wait_recv()
    build(o, 0, 2)
    for d in range(1, N_TP):
        ref = modall.at[(tp + N_TP - d) % N_TP]
        remote(ref, ref, m2_send.at[d], m2_recv.at[d], sp, pair).wait_recv()

    def mod_row(i):
        return jnp.concatenate([modall[t, pl.ds(i, 1), :] for t in range(N_TP)], axis=1)

    g = gain[...].reshape(1, D)
    for s in range(2):
        gate[s : s + 1] = mod_row(6 + s)
    shift, scaled = mod_row(c), g * (1.0 + mod_row(3 + c))
    ctx_shift, ctx_scaled = mod_row(2), g * (1.0 + mod_row(5))

    for cp in local[3:8]:
        cp.wait()
    hid[0:64] = modulated(ctx[...], ctx_scaled, ctx_shift)
    for cp in theirs[1:4]:
        cp.wait_recv()
    for j in range(2):
        for kind in range(2):
            ckv[j, kind, z, x] = jnp.dot(
                hid[0:64], wbuf[j, 1 + kind], preferred_element_type=F32
            ).astype(BF16)
    first = []
    for d in (2, 1, 3):
        own = ckv.at[0, :, z, x]
        first.append(
            remote(own, own, ca_send.at[d - 1], ca_recv.at[d - 1], 4 * z + (x + d) % 4, tp)
        )
        own = ckv.at[1, :, z, x]
        first.append(
            remote(own, own, ca_send.at[d + 2], ca_recv.at[d + 2], 4 * ((z + d) % 4) + x, tp)
        )
    for cp in first:
        cp.start()

    def keys_values(at):
        for kind in (1, 2):
            for j in range(2):
                kv[kind - 1, at, 256 * j : 256 * (j + 1)] = jnp.dot(
                    hid[...], wbuf[j, kind], preferred_element_type=F32
                ).astype(BF16)

    def unit(yy, k):
        for r in range(2):
            hid[64 * r : 64 * (r + 1)] = modulated(lat[2 * yy + r], scaled, shift)
        rows_q = pl.ds(pl.multiple_of(yy * 128, 128), 128)
        rows_k = pl.ds(pl.multiple_of(256 + yy * 128, 128), 128)
        hi = yy // 2
        to = pl.multiple_of(128 * (yy - 2 * hi) + 768 * (1 - hi), 128)
        cp = None if k == 0 else remote(
            kv.at[:, rows_k, :],
            kv.at[:, pl.ds(to, 128), :],
            h_send.at[k],
            h_recv.at[yy],
            (sp + 2 * hi - 1 + N_SP) % N_SP,
            tp,
        )
        to_sp = sp + 2 * hi - 1
        inner = (to_sp >= 0) & (to_sp < N_SP)
        keys_values(rows_k)
        for j in range(2):
            r = jnp.dot(hid[...], wbuf[j, 0], preferred_element_type=F32)
            q[rows_q, 256 * j : 256 * (j + 1)] = (r * (0.125 * LOG2E)).astype(BF16)
        return inner, cp

    def start_halo(halo):
        pl.when(halo[0])(halo[1].start)

    def arrived(ref, send, recv):
        remote(ref, ref, send, recv, sp, pair).wait_recv()

    def lat_wait(row, slot):
        arrived(lat.at[row], lat_send.at[slot], lat_recv.at[slot])

    lat_wait(2 * y + o, 0)
    unit(y, 0)
    halos = []
    build(o, 2, 4)

    lat_wait(2 * down, 1)
    ref = lat.at[2 * down]
    lats.append(remote(ref, ref, lat_send.at[5], lat_recv.at[5], sp, 2 * up + c))
    lats[-1].start()
    lat_wait(2 * up + 1, 4)
    ref = lat.at[2 * up + 1]
    lats.append(remote(ref, ref, lat_send.at[6], lat_recv.at[6], sp, 2 * down + c))
    lats[-1].start()

    for d in range(1, 4):
        arrived(ckv.at[0, :, z, (x + 4 - d) % 4], ca_send.at[d - 1], ca_recv.at[d - 1])
        arrived(ckv.at[1, :, (z + 4 - d) % 4, x], ca_send.at[d + 2], ca_recv.at[d + 2])
    routes = [
        (4 * z_up + x, ckv.at[0, :, z, 0:2], ckv.at[0, :, z, 2:4]),
        (4 * z_down + x, ckv.at[0, :, z, 2:4], ckv.at[0, :, z, 0:2]),
        (4 * z + x_up, ckv.at[1, :, 0:2, x], ckv.at[1, :, 2:4, x]),
        (4 * z + x_down, ckv.at[1, :, 2:4, x], ckv.at[1, :, 0:2, x]),
    ]
    second = []
    for part_of in range(2):
        for i, (to, *halves) in enumerate(routes):
            ref, k = halves[part_of], 4 * part_of + i
            cp = remote(ref, ref, cb_send.at[k], cb_recv.at[k], to, tp)
            cp.start()
            second.append(cp)

    lat_wait(2 * down + 1, 2)
    halos.append(unit(down, 1))
    lat_wait(2 * up, 3)
    halos.append(unit(up, 2))

    @pl.when(raw_in)
    def _():
        for r in range(2):
            arrived(hlat.at[r], raw_send.at[r], raw_recv.at[r])
            hid[64 * r : 64 * (r + 1)] = modulated(hlat[r], scaled, shift)
        keys_values(pl.ds(pl.multiple_of(128 * (y - 2 * own_hi) + 768 * (1 - own_hi), 128), 128))

    z_opp, x_opp = (z + 2) % 4, (x + 2) % 4
    passed = [
        (ckv.at[0, :, z_down, 0:2], 4 * z_up + x),
        (ckv.at[0, :, z_up, 2:4], 4 * z_down + x),
        (ckv.at[1, :, 0:2, x_down], 4 * z + x_up),
        (ckv.at[1, :, 2:4, x_up], 4 * z + x_down),
    ]
    for i, (half, to) in enumerate(passed):
        arrived(half, cb_send.at[i], cb_recv.at[i])
        cp = remote(half, half, cb_send.at[8 + i], cb_recv.at[8 + i], to, tp)
        cp.start()
        second.append(cp)
    for halo in halos:
        start_halo(halo)

    lat_wait(2 * opp, 5)
    lat_wait(2 * opp + 1, 6)
    halos.append(unit(opp, 3))
    start_halo(halos[-1])

    rest = [
        ckv.at[0, :, z_down, 2:4],
        ckv.at[0, :, z_up, 0:2],
        ckv.at[1, :, 2:4, x_down],
        ckv.at[1, :, 0:2, x_up],
        ckv.at[0, :, z_opp, 0:2],
        ckv.at[0, :, z_opp, 2:4],
        ckv.at[1, :, 0:2, x_opp],
        ckv.at[1, :, 2:4, x_opp],
    ]
    for i in range(4):
        arrived(rest[i], cb_send.at[4 + i], cb_recv.at[4 + i])

    ones_near = jnp.ones((512, 128), BF16)
    left = lax.broadcasted_iota(jnp.int32, (512, 128), 1) < W

    def far(zs, xs, again):
        for hp in range(4):
            lanes = slice(128 * hp, 128 * (hp + 1))
            within = slice(128 * (hp % 2), 128 * (hp % 2 + 1))

            def tokens(kind):
                if hp < 2:
                    blocks = [ckv[0, kind, k, :, :, within].reshape(256, 128) for k in zs]
                else:
                    blocks = [ckv[1, kind, :, k, :, within].reshape(256, 128) for k in xs]
                return jnp.concatenate(blocks, axis=0)

            qp, kp = q[:, lanes], tokens(0)
            vp = jnp.concatenate([tokens(1), jnp.ones((256 * len(zs), 128), BF16)], axis=1)
            for half in range(2):
                h = 2 * hp + half
                qh = jnp.where(left if half == 0 else ~left, qp, jnp.zeros_like(qp))
                s = lax.dot_general(qh, kp, (((1,), (1,)), ((), ())), preferred_element_type=F32)
                m = jnp.max(s, axis=-1, keepdims=True)
                if not again:
                    p = jnp.exp2(s - m).astype(BF16)
                    far_o[h] = jnp.dot(p, vp, preferred_element_type=F32)
                    far_m[h] = jnp.broadcast_to(m, (512, 128))
                    continue
                m_old = far_m[h]
                m = jnp.maximum(m, m_old)
                alpha = jnp.exp2(m_old - m)
                p = jnp.exp2(s - jnp.concatenate([m] * 2, axis=1)).astype(BF16)
                o_new = jnp.dot(p, vp, preferred_element_type=F32)
                far_o[h, :, :128] = o_new[:, :128] + alpha * far_o[h, :, :128]
                far_o[h, :, 128:] = o_new[:, 128:] + alpha * far_o[h, :, 128:]
                far_m[h] = m + rel[h // 4, 15, h % 4 : h % 4 + 1, :] * LOG2E

    far((z, z_up, z_down), (x, x_up, x_down), False)
    for i in range(4, 8):
        arrived(rest[i], cb_send.at[4 + i], cb_recv.at[4 + i])
    far((z_opp,), (x_opp,), True)

    def halo_wait(yy):
        hi = yy // 2
        at = pl.ds(pl.multiple_of(128 * (yy - 2 * hi) + 768 * (1 - hi), 128), 128)
        of_sp = sp + 1 - 2 * hi

        @pl.when((of_sp >= 0) & (of_sp < N_SP))
        def _():
            arrived(kv.at[:, at, :], h_send.at[yy], h_recv.at[yy])

    for yy in (up, down):
        halo_wait(yy)
    theirs[4].wait_recv()
    local[8].wait()

    def near(yy):
        def one(r, carry):
            row = 2 * yy + r
            g = sp * 8 + row
            r0 = jnp.clip(g - 4, 0, 120)
            base = pl.multiple_of((r0 - sp * 8 + 4) * W, W)
            a0 = r0 - g + 7
            at = pl.ds(pl.multiple_of(row * W, W), W)
            for hp in range(4):
                lanes = slice(128 * hp, 128 * (hp + 1))
                qp = q[at, lanes]
                kp = kv[0, pl.ds(base, 512), lanes]
                vp = jnp.concatenate([kv[1, pl.ds(base, 512), lanes], ones_near], axis=1)
                outs = []
                for half in range(2):
                    h = 2 * hp + half
                    own = lane < W if half == 0 else lane >= W
                    qh = jnp.where(own, qp, jnp.zeros_like(qp))
                    s = lax.dot_general(qh, kp, (((1,), (1,)), ((), ())), preferred_element_type=F32)
                    s = s + jnp.concatenate([table[h, a0 + 2 * k] for k in range(4)], axis=1)
                    m1 = far_m[h, at, :]
                    m = jnp.maximum(jnp.max(s, axis=-1, keepdims=True), m1)
                    alpha = jnp.exp2(m1 - m)
                    p = jnp.exp2(s - jnp.concatenate([m] * 4, axis=1)).astype(BF16)
                    close = jnp.dot(p, vp, preferred_element_type=F32)
                    top = close[:, :128] + alpha * far_o[h, at, :128]
                    total = close[:, 128:] + alpha * far_o[h, at, 128:]
                    outs.append(top / total)
                att[pl.ds(pl.multiple_of(r * W, W), W), lanes] = jnp.where(
                    lane < W, outs[0], outs[1]
                ).astype(BF16)
            return carry

        lax.fori_loop(0, 2, one, 0)
        full = wout[...].reshape(512, D)
        part[yy] = jnp.dot(att[...], full, preferred_element_type=F32).astype(BF16)

    def row(yy, r):
        return part.at[yy, pl.ds(pl.multiple_of(r * W, W), W), :]

    def send(k, src, slot, to):
        cp = remote(src, inbox.at[c, slot], i_send.at[k], i_recv.at[c, slot], sp, to)
        cp.start()
        return cp

    near(opp)
    relays = [
        remote(row(opp, 0), relay.at[0], r_send.at[0], r_recv.at[0], sp, 2 * up + c),
        remote(row(opp, 1), relay.at[1], r_send.at[1], r_recv.at[1], sp, 2 * down + c),
    ]
    for cp in relays:
        cp.start()
    e = y // 2
    second_y, third_y = (y + 1 + 2 * e) % 4, (y + 3 + 2 * e) % 4
    near(second_y)
    sends = [send(0, row(second_y, 1 - e), e, 2 * second_y + 1 - e)]
    halo_wait(opp)
    near(third_y)
    sends.append(send(1, row(third_y, e), 1 - e, 2 * third_y + e))
    near(y)
    sends.append(send(2, row(y, o), 2, pair))
    inbox[c, 2] = part[y, pl.ds(pl.multiple_of(c * W, W), W), :]
    for k, yy, r in ((3, second_y, e), (4, third_y, 1 - e)):
        arrived(relay.at[r], r_send.at[r], r_recv.at[r])
        mine_too = part[yy, pl.ds(pl.multiple_of(r * W, W), W), :]
        comb[r] = (mine_too.astype(F32) + relay[r].astype(F32)).astype(BF16)
        sends.append(send(k, comb.at[r], r, 2 * yy + r))

    def got(s, k):
        arrived(inbox.at[s, k], i_send.at[k], i_recv.at[s, k])

    local[9].wait()
    got(o, 2)
    for s in range(2):
        got(s, 0)
        got(s, 1)
    for s in range(2):
        update = inbox[s, 0].astype(F32) + inbox[s, 1].astype(F32) + inbox[s, 2].astype(F32)
        out[s] = (mine[s].astype(F32) + gate[s : s + 1] * update).astype(BF16)
    for cp in lats + weights + m1 + m2 + first + second + relays + sends:
        cp.wait_send()
    for inner, cp in halos:
        pl.when(inner)(cp.wait_send)

    @pl.when(raw_out)
    def _():
        for cp in raws:
            cp.wait_send()


VM = pl.BlockSpec(memory_space=pltpu.VMEM)
SM = pl.BlockSpec(memory_space=pltpu.SMEM)
ANY = pl.BlockSpec(memory_space=pltpu.HBM)
DMA = pltpu.SemaphoreType.DMA


def on_device(*args):
    args = [*args[:12], args[12].transpose(1, 0, 2), args[13]]
    args = [pltpu.with_memory_space_constraint(a, pltpu.HBM) for a in args]
    return pl.pallas_call(
        kernel,
        out_shape=jax.ShapeDtypeStruct((2, W, D), BF16),
        in_specs=[ANY, ANY, VM, VM, ANY, ANY, ANY, VM, ANY, ANY, ANY, ANY, VM, SM],
        out_specs=VM,
        scratch_shapes=[
            pltpu.VMEM((512, 512), BF16),
            pltpu.VMEM((2, 1024, 512), BF16),
            pltpu.VMEM((2, 2, NZ, NX, 64, 256), BF16),
            pltpu.VMEM((2, 256, D), BF16),
            pltpu.VMEM((2, 16, 4, 128), F32),
            pltpu.VMEM((2, D), F32),
            pltpu.VMEM((8, W, D), BF16),
            pltpu.VMEM((W, D), BF16),
            pltpu.VMEM((3, 128, 256), BF16),
            pltpu.VMEM((2, 3, D, 256), BF16),
            pltpu.VMEM((8, 128), F32),
            pltpu.VMEM((1, D), F32),
            pltpu.VMEM((16, 8, 256), F32),
            pltpu.VMEM((8, 8, 256), F32),
            pltpu.VMEM((128, D), BF16),
            pltpu.VMEM((8, 14, W, 128), F32),
            pltpu.VMEM((8, 512, 256), F32),
            pltpu.VMEM((8, 512, 128), F32),
            pltpu.VMEM((128, 512), BF16),
            pltpu.VMEM((4, 128, D), BF16),
            pltpu.VMEM((2, W, D), BF16),
            pltpu.VMEM((2, W, D), BF16),
            pltpu.VMEM((2, 3, W, D), BF16),
            pltpu.VMEM((2, W, D), BF16),
            pltpu.VMEM((2, W, D), BF16),
            DMA((10,)),
            DMA((5,)), DMA((5,)), DMA((7,)), DMA((7,)),
            DMA((16,)), DMA((16,)), DMA((8,)), DMA((8,)),
            DMA((6,)), DMA((6,)), DMA((12,)), DMA((12,)), DMA((4,)), DMA((4,)),
            DMA((2,)), DMA((2,)), DMA((5,)), DMA((2, 3)), DMA((2,)), DMA((2,)),
        ],
        compiler_params=pltpu.CompilerParams(
            collective_id=0, has_side_effects=True, vmem_limit_bytes=48 * 2**20
        ),
        name="layer",
    )(*args)


def solution(mesh):
    return jax.shard_map(
        on_device,
        mesh=mesh,
        in_specs=(
            P(None, ("sp", "tp"), None),
            P(None, "sp", None),
            P(),
            P(),
            P("sp", "tp"),
            P("sp", "tp"),
            P("sp", "tp"),
            P(),
            P(None, "tp"),
            P(None, "tp"),
            P(None, "tp"),
            P("tp", None),
            P("tp", None, None),
            P("tp"),
        ),
        out_specs=P(None, ("sp", "tp"), None),
        check_vma=False,
    )
```

```python
import functools

import jax
import jax.numpy as jnp
from jax import lax
from jax.experimental import pallas as pl
from jax.experimental.pallas import tpu as pltpu
from jax.sharding import PartitionSpec as P

MESH = pl.DeviceIdType.MESH
F32, BF16 = jnp.float32, jnp.bfloat16
N_SP, N_TP, NX, NZ, NY = 16, 8, 4, 4, 4
D = 2048
W = 64
EPSILON = 1e-06
LOG2E = 1.4426950408889634
MASKED = -1e30


def silu(v):
    return v / (1.0 + jnp.exp(-v))


def modulated(x, gain, shift):
    f = x.astype(F32)
    inv = lax.rsqrt(jnp.mean(f * f, axis=-1, keepdims=True) + EPSILON)
    return (f * inv * gain + shift).astype(BF16)


def remote(src, dst, send, recv, sp, tp):
    return pltpu.make_async_remote_copy(
        src_ref=src, dst_ref=dst, send_sem=send, recv_sem=recv, device_id=(sp, tp), device_id_type=MESH
    )


def kernel(
    latent, context, cond, ctx_cond, wsh, wsc, wga, gain, wq, wk, wv, wo, rel_bias, ctx_bias,
    out,
    q, kv, ckv, wout, rel, gate, lat, ctx, wmod, wbuf, ada, ctx_ada, modrecv, modall, hid,
    table, far_o, far_m, att, part, relay, comb, inbox, mine,
    loc_sem, w_send, w_recv, lat_send, lat_recv, m1_send, m1_recv, m2_send, m2_recv,
    ca_send, ca_recv, cb_send, cb_recv, h_send, h_recv, r_send, r_recv, i_send, i_recv,
):
    sp, tp = lax.axis_index("sp"), lax.axis_index("tp")
    y, c = tp // 2, tp % 2
    z, x = sp // 4, sp % 4
    o = 1 - c
    pair = tp + 1 - 2 * c
    up, down, opp = (y + 1) % 4, (y + 3) % 4, (y + 2) % 4
    z_up, z_down, x_up, x_down = (z + 1) % 4, (z + 3) % 4, (x + 1) % 4, (x + 3) % 4

    barrier = pltpu.get_barrier_semaphore()
    for d in range(1, N_SP):
        pl.semaphore_signal(barrier, inc=1, device_id=((sp + d) % N_SP, tp), device_id_type=MESH)
    for d in range(1, N_TP):
        pl.semaphore_signal(barrier, inc=1, device_id=(sp, (tp + d) % N_TP), device_id_type=MESH)

    local = [
        pltpu.make_async_copy(wsh, wmod.at[0], loc_sem.at[0]),
        pltpu.make_async_copy(wsc, wmod.at[1], loc_sem.at[1]),
        pltpu.make_async_copy(wga, wmod.at[2], loc_sem.at[2]),
        pltpu.make_async_copy(context.at[c], ctx, loc_sem.at[3]),
        pltpu.make_async_copy(latent.at[c], lat.at[tp], loc_sem.at[4]),
        pltpu.make_async_copy(wk, wbuf.at[c, 1], loc_sem.at[5]),
        pltpu.make_async_copy(wv, wbuf.at[c, 2], loc_sem.at[6]),
        pltpu.make_async_copy(wq, wbuf.at[c, 0], loc_sem.at[7]),
        pltpu.make_async_copy(wo, wout.at[c], loc_sem.at[8]),
        pltpu.make_async_copy(latent, mine, loc_sem.at[9]),
    ]
    for cp in local:
        cp.start()
    rel[c] = jnp.zeros((16, 4, 128), F32)
    rel[c, 0:14, :, 0:31] = rel_bias[0:14]
    rel[c, 0:14, :, 64:95] = rel_bias[1:15]
    for h in range(4):
        rel[c, 15, h : h + 1, :] = jnp.full((1, 128), ctx_bias[h], F32)

    at = pl.ds(pl.multiple_of(sp * 128, 128), 128)
    ada[...] = jnp.zeros_like(ada)
    ada[0:2] = silu(cond[:, at].astype(F32))
    ctx_ada[...] = silu(ctx_cond[...].astype(F32)).reshape(1, D)
    ada[2:3] = ctx_ada[:, at]
    rows = ada[...].astype(BF16)
    for cp in local[:3]:
        cp.wait()
    sums = [jnp.dot(rows, wmod[i], preferred_element_type=F32) for i in range(3)]
    modrecv[0, 0:3] = sums[0][0:3]
    modrecv[0, 3:6] = sums[1][0:3]
    modrecv[0, 6:8] = sums[2][0:2]

    pl.semaphore_wait(barrier, N_SP + N_TP - 2)

    m1 = [
        remote(modrecv.at[0], modrecv.at[d], m1_send.at[d], m1_recv.at[d], (sp + d) % N_SP, tp)
        for d in range(1, N_SP)
    ]

    def lat_copy(s, k, yy, j, slot):
        return remote(latent.at[s], lat.at[tp], lat_send.at[k], lat_recv.at[slot], sp, 2 * yy + j)

    ahead, behind = (y + 1 + 2 * c) % 4, (y + 3 + 2 * c) % 4
    lats = [
        lat_copy(o, 4, y, o, 0),
        lat_copy(c, 0, ahead, c, 1 + 3 * c),
        lat_copy(o, 2, ahead, o, 1 + 3 * c),
        lat_copy(c, 1, behind, c, 3 - c),
        lat_copy(o, 3, behind, o, 3 - c),
    ]

    def weight_copies(j):
        pairs = [
            (rel.at[j], rel.at[j]),
            (wk if j is c else wbuf.at[j, 1], wbuf.at[j, 1]),
            (wv if j is c else wbuf.at[j, 2], wbuf.at[j, 2]),
            (wq if j is c else wbuf.at[j, 0], wbuf.at[j, 0]),
            (wo if j is c else wout.at[j], wout.at[j]),
        ]
        return [
            remote(a, b, w_send.at[i], w_recv.at[i], sp, pair) for i, (a, b) in enumerate(pairs)
        ]

    weights, theirs = weight_copies(c), weight_copies(o)
    for cp in m1 + weights[:1] + lats[:2] + weights[1:]:
        cp.start()

    lane = lax.broadcasted_iota(jnp.int32, (W, 128), 1)
    col = lax.broadcasted_iota(jnp.int32, (W, 128), 0)
    key = lane % W
    start = jnp.clip(col - 8, 0, 48)
    inside = (key >= start) & (key < start + 16)

    def build(j, first, last):
        def one(h, carry):
            for a in range(14):
                r = jnp.broadcast_to(rel[j, a, pl.ds(h, 1), :] * LOG2E, (W, 128))
                r = pltpu.roll(r, 113, 1, stride=1, stride_axis=0)
                table[4 * j + h, a] = jnp.where(inside, r, MASKED)
            return carry

        lax.fori_loop(first, last, one, 0)

    build(c, 0, 4)

    for cp in m1:
        cp.wait_recv()
    modall[tp] = jnp.sum(modrecv[...], axis=0)
    m2 = [
        remote(modall.at[tp], modall.at[tp], m2_send.at[d], m2_recv.at[d], sp, (tp + d) % N_TP)
        for d in range(1, N_TP)
    ]
    for cp in m2 + lats[2:]:
        cp.start()
    theirs[0].wait_recv()
    build(o, 0, 2)
    for d in range(1, N_TP):
        ref = modall.at[(tp + N_TP - d) % N_TP]
        remote(ref, ref, m2_send.at[d], m2_recv.at[d], sp, pair).wait_recv()

    def mod_row(i):
        return jnp.concatenate([modall[t, pl.ds(i, 1), :] for t in range(N_TP)], axis=1)

    g = gain[...].reshape(1, D)
    for s in range(2):
        gate[s : s + 1] = mod_row(6 + s)
    shift, scaled = mod_row(c), g * (1.0 + mod_row(3 + c))
    ctx_shift, ctx_scaled = mod_row(2), g * (1.0 + mod_row(5))

    for cp in local[3:8]:
        cp.wait()
    hid[0:64] = modulated(ctx[...], ctx_scaled, ctx_shift)
    for cp in theirs[1:4]:
        cp.wait_recv()
    for j in range(2):
        for kind in range(2):
            ckv[j, kind, z, x] = jnp.dot(
                hid[0:64], wbuf[j, 1 + kind], preferred_element_type=F32
            ).astype(BF16)
    first = []
    for d in (2, 1, 3):
        own = ckv.at[0, :, z, x]
        first.append(
            remote(own, own, ca_send.at[d - 1], ca_recv.at[d - 1], 4 * z + (x + d) % 4, tp)
        )
        own = ckv.at[1, :, z, x]
        first.append(
            remote(own, own, ca_send.at[d + 2], ca_recv.at[d + 2], 4 * ((z + d) % 4) + x, tp)
        )
    for cp in first:
        cp.start()

    def unit(yy, k):
        for r in range(2):
            hid[64 * r : 64 * (r + 1)] = modulated(lat[2 * yy + r], scaled, shift)
        rows_q = pl.ds(pl.multiple_of(yy * 128, 128), 128)
        rows_k = pl.ds(pl.multiple_of(256 + yy * 128, 128), 128)
        hi = yy // 2
        to = pl.multiple_of(128 * (yy - 2 * hi) + 768 * (1 - hi), 128)
        cp = remote(
            kv.at[:, rows_k, :],
            kv.at[:, pl.ds(to, 128), :],
            h_send.at[k],
            h_recv.at[yy],
            (sp + 2 * hi - 1 + N_SP) % N_SP,
            tp,
        )
        to_sp = sp + 2 * hi - 1
        inner = (to_sp >= 0) & (to_sp < N_SP)
        for kind in (1, 2, 0):
            for j in range(2):
                cols = slice(256 * j, 256 * (j + 1))
                r = jnp.dot(hid[...], wbuf[j, kind], preferred_element_type=F32)
                if kind == 0:
                    q[rows_q, cols] = (r * (0.125 * LOG2E)).astype(BF16)
                else:
                    kv[kind - 1, rows_k, cols] = r.astype(BF16)
        return inner, cp

    def start_halo(halo):
        pl.when(halo[0])(halo[1].start)

    def arrived(ref, send, recv):
        remote(ref, ref, send, recv, sp, pair).wait_recv()

    def lat_wait(row, slot):
        arrived(lat.at[row], lat_send.at[slot], lat_recv.at[slot])

    lat_wait(2 * y + o, 0)
    halos = [unit(y, 0)]
    start_halo(halos[0])
    build(o, 2, 4)

    lat_wait(2 * down, 1)
    ref = lat.at[2 * down]
    lats.append(remote(ref, ref, lat_send.at[5], lat_recv.at[5], sp, 2 * up + c))
    lats[-1].start()
    lat_wait(2 * up + 1, 4)
    ref = lat.at[2 * up + 1]
    lats.append(remote(ref, ref, lat_send.at[6], lat_recv.at[6], sp, 2 * down + c))
    lats[-1].start()

    for d in range(1, 4):
        arrived(ckv.at[0, :, z, (x + 4 - d) % 4], ca_send.at[d - 1], ca_recv.at[d - 1])
        arrived(ckv.at[1, :, (z + 4 - d) % 4, x], ca_send.at[d + 2], ca_recv.at[d + 2])
    routes = [
        (4 * z_up + x, ckv.at[0, :, z, 0:2], ckv.at[0, :, z, 2:4]),
        (4 * z_down + x, ckv.at[0, :, z, 2:4], ckv.at[0, :, z, 0:2]),
        (4 * z + x_up, ckv.at[1, :, 0:2, x], ckv.at[1, :, 2:4, x]),
        (4 * z + x_down, ckv.at[1, :, 2:4, x], ckv.at[1, :, 0:2, x]),
    ]
    second = []
    for part_of in range(2):
        for i, (to, *halves) in enumerate(routes):
            ref, k = halves[part_of], 4 * part_of + i
            cp = remote(ref, ref, cb_send.at[k], cb_recv.at[k], to, tp)
            cp.start()
            second.append(cp)

    lat_wait(2 * down + 1, 2)
    halos.append(unit(down, 1))
    lat_wait(2 * up, 3)
    halos.append(unit(up, 2))

    z_opp, x_opp = (z + 2) % 4, (x + 2) % 4
    passed = [
        (ckv.at[0, :, z_down, 0:2], 4 * z_up + x),
        (ckv.at[0, :, z_up, 2:4], 4 * z_down + x),
        (ckv.at[1, :, 0:2, x_down], 4 * z + x_up),
        (ckv.at[1, :, 2:4, x_up], 4 * z + x_down),
    ]
    for i, (half, to) in enumerate(passed):
        arrived(half, cb_send.at[i], cb_recv.at[i])
        cp = remote(half, half, cb_send.at[8 + i], cb_recv.at[8 + i], to, tp)
        cp.start()
        second.append(cp)
    for halo in halos[1:]:
        start_halo(halo)

    lat_wait(2 * opp, 5)
    lat_wait(2 * opp + 1, 6)
    halos.append(unit(opp, 3))
    start_halo(halos[-1])

    rest = [
        ckv.at[0, :, z_down, 2:4],
        ckv.at[0, :, z_up, 0:2],
        ckv.at[1, :, 2:4, x_down],
        ckv.at[1, :, 0:2, x_up],
        ckv.at[0, :, z_opp, 0:2],
        ckv.at[0, :, z_opp, 2:4],
        ckv.at[1, :, 0:2, x_opp],
        ckv.at[1, :, 2:4, x_opp],
    ]
    for i in range(4):
        arrived(rest[i], cb_send.at[4 + i], cb_recv.at[4 + i])

    ones_near = jnp.ones((512, 128), BF16)
    left = lax.broadcasted_iota(jnp.int32, (512, 128), 1) < W

    def far(zs, xs, again):
        for hp in range(4):
            lanes = slice(128 * hp, 128 * (hp + 1))
            within = slice(128 * (hp % 2), 128 * (hp % 2 + 1))

            def tokens(kind):
                if hp < 2:
                    blocks = [ckv[0, kind, k, :, :, within].reshape(256, 128) for k in zs]
                else:
                    blocks = [ckv[1, kind, :, k, :, within].reshape(256, 128) for k in xs]
                return jnp.concatenate(blocks, axis=0)

            qp, kp = q[:, lanes], tokens(0)
            vp = jnp.concatenate([tokens(1), jnp.ones((256 * len(zs), 128), BF16)], axis=1)
            for half in range(2):
                h = 2 * hp + half
                qh = jnp.where(left if half == 0 else ~left, qp, jnp.zeros_like(qp))
                s = lax.dot_general(qh, kp, (((1,), (1,)), ((), ())), preferred_element_type=F32)
                m = jnp.max(s, axis=-1, keepdims=True)
                if not again:
                    p = jnp.exp2(s - m).astype(BF16)
                    far_o[h] = jnp.dot(p, vp, preferred_element_type=F32)
                    far_m[h] = jnp.broadcast_to(m, (512, 128))
                    continue
                m_old = far_m[h]
                m = jnp.maximum(m, m_old)
                alpha = jnp.exp2(m_old - m)
                p = jnp.exp2(s - jnp.concatenate([m] * 2, axis=1)).astype(BF16)
                o_new = jnp.dot(p, vp, preferred_element_type=F32)
                far_o[h, :, :128] = o_new[:, :128] + alpha * far_o[h, :, :128]
                far_o[h, :, 128:] = o_new[:, 128:] + alpha * far_o[h, :, 128:]
                far_m[h] = m + rel[h // 4, 15, h % 4 : h % 4 + 1, :] * LOG2E

    far((z, z_up, z_down), (x, x_up, x_down), False)
    for i in range(4, 8):
        arrived(rest[i], cb_send.at[4 + i], cb_recv.at[4 + i])
    far((z_opp,), (x_opp,), True)

    def halo_wait(yy):
        hi = yy // 2
        at = pl.ds(pl.multiple_of(128 * (yy - 2 * hi) + 768 * (1 - hi), 128), 128)
        of_sp = sp + 1 - 2 * hi

        @pl.when((of_sp >= 0) & (of_sp < N_SP))
        def _():
            arrived(kv.at[:, at, :], h_send.at[yy], h_recv.at[yy])

    for yy in (y, up, down):
        halo_wait(yy)
    theirs[4].wait_recv()
    local[8].wait()

    def near(yy):
        def one(r, carry):
            row = 2 * yy + r
            g = sp * 8 + row
            r0 = jnp.clip(g - 4, 0, 120)
            base = pl.multiple_of((r0 - sp * 8 + 4) * W, W)
            a0 = r0 - g + 7
            at = pl.ds(pl.multiple_of(row * W, W), W)
            for hp in range(4):
                lanes = slice(128 * hp, 128 * (hp + 1))
                qp = q[at, lanes]
                kp = kv[0, pl.ds(base, 512), lanes]
                vp = jnp.concatenate([kv[1, pl.ds(base, 512), lanes], ones_near], axis=1)
                zero = jnp.zeros_like(qp)
                qs = jnp.concatenate(
                    [jnp.where(lane < W, qp, zero), jnp.where(lane < W, zero, qp)], axis=0
                )
                s = lax.dot_general(qs, kp, (((1,), (1,)), ((), ())), preferred_element_type=F32)

                def of_pair(get):
                    return jnp.concatenate([get(2 * hp), get(2 * hp + 1)], axis=0)

                s = s + of_pair(
                    lambda h: jnp.concatenate([table[h, a0 + 2 * k] for k in range(4)], axis=1)
                )
                m1 = of_pair(lambda h: far_m[h, at, :])
                m = jnp.maximum(jnp.max(s, axis=-1, keepdims=True), m1)
                alpha = jnp.exp2(m1 - m)
                p = jnp.exp2(s - jnp.concatenate([m] * 4, axis=1)).astype(BF16)
                close = jnp.dot(p, vp, preferred_element_type=F32)
                top = close[:, :128] + alpha * of_pair(lambda h: far_o[h, at, :128])
                total = close[:, 128:] + alpha * of_pair(lambda h: far_o[h, at, 128:])
                both = top / total
                att[pl.ds(pl.multiple_of(r * W, W), W), lanes] = jnp.where(
                    lane < W, both[:W], both[W:]
                ).astype(BF16)
            return carry

        lax.fori_loop(0, 2, one, 0)
        full = wout[...].reshape(512, D)
        part[yy] = jnp.dot(att[...], full, preferred_element_type=F32).astype(BF16)

    def row(yy, r):
        return part.at[yy, pl.ds(pl.multiple_of(r * W, W), W), :]

    def send(k, src, slot, to):
        cp = remote(src, inbox.at[c, slot], i_send.at[k], i_recv.at[c, slot], sp, to)
        cp.start()
        return cp

    near(opp)
    relays = [
        remote(row(opp, 0), relay.at[0], r_send.at[0], r_recv.at[0], sp, 2 * up + c),
        remote(row(opp, 1), relay.at[1], r_send.at[1], r_recv.at[1], sp, 2 * down + c),
    ]
    for cp in relays:
        cp.start()
    e = y // 2
    second_y, third_y = (y + 1 + 2 * e) % 4, (y + 3 + 2 * e) % 4
    near(second_y)
    sends = [send(0, row(second_y, 1 - e), e, 2 * second_y + 1 - e)]
    halo_wait(opp)
    near(third_y)
    sends.append(send(1, row(third_y, e), 1 - e, 2 * third_y + e))
    near(y)
    sends.append(send(2, row(y, o), 2, pair))
    inbox[c, 2] = part[y, pl.ds(pl.multiple_of(c * W, W), W), :]
    for k, yy, r in ((3, second_y, e), (4, third_y, 1 - e)):
        arrived(relay.at[r], r_send.at[r], r_recv.at[r])
        mine_too = part[yy, pl.ds(pl.multiple_of(r * W, W), W), :]
        comb[r] = (mine_too.astype(F32) + relay[r].astype(F32)).astype(BF16)
        sends.append(send(k, comb.at[r], r, 2 * yy + r))

    def got(s, k):
        arrived(inbox.at[s, k], i_send.at[k], i_recv.at[s, k])

    local[9].wait()
    got(o, 2)
    for s in range(2):
        got(s, 0)
        got(s, 1)
    for s in range(2):
        update = inbox[s, 0].astype(F32) + inbox[s, 1].astype(F32) + inbox[s, 2].astype(F32)
        out[s] = (mine[s].astype(F32) + gate[s : s + 1] * update).astype(BF16)
    for cp in lats + weights + m1 + m2 + first + second + relays + sends:
        cp.wait_send()
    for inner, cp in halos:
        pl.when(inner)(cp.wait_send)


VM = pl.BlockSpec(memory_space=pltpu.VMEM)
SM = pl.BlockSpec(memory_space=pltpu.SMEM)
ANY = pl.BlockSpec(memory_space=pltpu.HBM)
DMA = pltpu.SemaphoreType.DMA


def on_device(*args):
    args = [*args[:12], args[12].transpose(1, 0, 2), args[13]]
    args = [pltpu.with_memory_space_constraint(a, pltpu.HBM) for a in args]
    return pl.pallas_call(
        kernel,
        out_shape=jax.ShapeDtypeStruct((2, W, D), BF16),
        in_specs=[ANY, ANY, VM, VM, ANY, ANY, ANY, VM, ANY, ANY, ANY, ANY, VM, SM],
        out_specs=VM,
        scratch_shapes=[
            pltpu.VMEM((512, 512), BF16),
            pltpu.VMEM((2, 1024, 512), BF16),
            pltpu.VMEM((2, 2, NZ, NX, 64, 256), BF16),
            pltpu.VMEM((2, 256, D), BF16),
            pltpu.VMEM((2, 16, 4, 128), F32),
            pltpu.VMEM((2, D), F32),
            pltpu.VMEM((8, W, D), BF16),
            pltpu.VMEM((W, D), BF16),
            pltpu.VMEM((3, 128, 256), BF16),
            pltpu.VMEM((2, 3, D, 256), BF16),
            pltpu.VMEM((8, 128), F32),
            pltpu.VMEM((1, D), F32),
            pltpu.VMEM((16, 8, 256), F32),
            pltpu.VMEM((8, 8, 256), F32),
            pltpu.VMEM((128, D), BF16),
            pltpu.VMEM((8, 14, W, 128), F32),
            pltpu.VMEM((8, 512, 256), F32),
            pltpu.VMEM((8, 512, 128), F32),
            pltpu.VMEM((128, 512), BF16),
            pltpu.VMEM((4, 128, D), BF16),
            pltpu.VMEM((2, W, D), BF16),
            pltpu.VMEM((2, W, D), BF16),
            pltpu.VMEM((2, 3, W, D), BF16),
            pltpu.VMEM((2, W, D), BF16),
            DMA((10,)),
            DMA((5,)), DMA((5,)), DMA((7,)), DMA((7,)),
            DMA((16,)), DMA((16,)), DMA((8,)), DMA((8,)),
            DMA((6,)), DMA((6,)), DMA((12,)), DMA((12,)), DMA((4,)), DMA((4,)),
            DMA((2,)), DMA((2,)), DMA((5,)), DMA((2, 3)),
        ],
        compiler_params=pltpu.CompilerParams(
            collective_id=0, has_side_effects=True, vmem_limit_bytes=48 * 2**20
        ),
        name="layer",
    )(*args)


def solution(mesh):
    return jax.shard_map(
        on_device,
        mesh=mesh,
        in_specs=(
            P(None, ("sp", "tp"), None),
            P(None, "sp", None),
            P(),
            P(),
            P("sp", "tp"),
            P("sp", "tp"),
            P("sp", "tp"),
            P(),
            P(None, "tp"),
            P(None, "tp"),
            P(None, "tp"),
            P("tp", None),
            P("tp", None, None),
            P("tp"),
        ),
        out_specs=P(None, ("sp", "tp"), None),
        check_vma=False,
    )
```

```python
import functools

import jax
import jax.numpy as jnp
from jax import lax
from jax.experimental import pallas as pl
from jax.experimental.pallas import tpu as pltpu
from jax.sharding import PartitionSpec as P

MESH = pl.DeviceIdType.MESH
F32, BF16 = jnp.float32, jnp.bfloat16
N_SP, N_TP, NX, NZ, NY = 16, 8, 4, 4, 4
D = 2048
W = 64
EPSILON = 1e-06
LOG2E = 1.4426950408889634
MASKED = -1e30


def silu(v):
    return v / (1.0 + jnp.exp(-v))


def modulated(x, gain, shift):
    f = x.astype(F32)
    inv = lax.rsqrt(jnp.mean(f * f, axis=-1, keepdims=True) + EPSILON)
    return (f * inv * gain + shift).astype(BF16)


def remote(src, dst, send, recv, sp, tp):
    return pltpu.make_async_remote_copy(
        src_ref=src, dst_ref=dst, send_sem=send, recv_sem=recv, device_id=(sp, tp), device_id_type=MESH
    )


def kernel(
    latent, context, cond, ctx_cond, wsh, wsc, wga, gain, wq, wk, wv, wo, rel_bias, ctx_bias,
    out,
    q, kv, ckv, wout, rel, gate, lat, ctx, wmod, wbuf, ada, ctx_ada, modrecv, modall, hid,
    table, far_o, far_m, att, part, relay, comb, inbox, mine, normed,
    loc_sem, w_send, w_recv, lat_send, lat_recv, m1_send, m1_recv, m2_send, m2_recv,
    ca_send, ca_recv, cb_send, cb_recv, h_send, h_recv, r_send, r_recv, i_send, i_recv,
):
    sp, tp = lax.axis_index("sp"), lax.axis_index("tp")
    y, c = tp // 2, tp % 2
    z, x = sp // 4, sp % 4
    o = 1 - c
    pair = tp + 1 - 2 * c
    up, down, opp = (y + 1) % 4, (y + 3) % 4, (y + 2) % 4
    z_up, z_down, x_up, x_down = (z + 1) % 4, (z + 3) % 4, (x + 1) % 4, (x + 3) % 4

    barrier = pltpu.get_barrier_semaphore()
    for d in range(1, N_SP):
        pl.semaphore_signal(barrier, inc=1, device_id=((sp + d) % N_SP, tp), device_id_type=MESH)
    for d in range(1, N_TP):
        pl.semaphore_signal(barrier, inc=1, device_id=(sp, (tp + d) % N_TP), device_id_type=MESH)

    local = [
        pltpu.make_async_copy(wsh, wmod.at[0], loc_sem.at[0]),
        pltpu.make_async_copy(wsc, wmod.at[1], loc_sem.at[1]),
        pltpu.make_async_copy(wga, wmod.at[2], loc_sem.at[2]),
        pltpu.make_async_copy(context.at[c], ctx, loc_sem.at[3]),
        pltpu.make_async_copy(latent.at[c], lat.at[tp], loc_sem.at[4]),
        pltpu.make_async_copy(wk, wbuf.at[c, 1], loc_sem.at[5]),
        pltpu.make_async_copy(wv, wbuf.at[c, 2], loc_sem.at[6]),
        pltpu.make_async_copy(wq, wbuf.at[c, 0], loc_sem.at[7]),
        pltpu.make_async_copy(wo, wout.at[c], loc_sem.at[8]),
        pltpu.make_async_copy(latent, mine, loc_sem.at[9]),
    ]
    for cp in local:
        cp.start()
    rel[c] = jnp.zeros((16, 4, 128), F32)
    rel[c, 0:14, :, 0:31] = rel_bias[0:14]
    rel[c, 0:14, :, 64:95] = rel_bias[1:15]
    for h in range(4):
        rel[c, 15, h : h + 1, :] = jnp.full((1, 128), ctx_bias[h], F32)

    at = pl.ds(pl.multiple_of(sp * 128, 128), 128)
    ada[...] = jnp.zeros_like(ada)
    ada[0:2] = silu(cond[:, at].astype(F32))
    ctx_ada[...] = silu(ctx_cond[...].astype(F32)).reshape(1, D)
    ada[2:3] = ctx_ada[:, at]
    rows = ada[...].astype(BF16)
    for cp in local[:3]:
        cp.wait()
    sums = [jnp.dot(rows, wmod[i], preferred_element_type=F32) for i in range(3)]
    modrecv[0, 0:3] = sums[0][0:3]
    modrecv[0, 3:6] = sums[1][0:3]
    modrecv[0, 6:8] = sums[2][0:2]

    pl.semaphore_wait(barrier, N_SP + N_TP - 2)

    m1 = [
        remote(modrecv.at[0], modrecv.at[d], m1_send.at[d], m1_recv.at[d], (sp + d) % N_SP, tp)
        for d in range(1, N_SP)
    ]

    def lat_copy(s, k, yy, j, slot):
        return remote(latent.at[s], lat.at[tp], lat_send.at[k], lat_recv.at[slot], sp, 2 * yy + j)

    ahead, behind = (y + 1 + 2 * c) % 4, (y + 3 + 2 * c) % 4
    lats = [
        lat_copy(o, 4, y, o, 0),
        lat_copy(c, 0, ahead, c, 1 + 3 * c),
        lat_copy(o, 2, ahead, o, 1 + 3 * c),
        lat_copy(c, 1, behind, c, 3 - c),
        lat_copy(o, 3, behind, o, 3 - c),
    ]

    def weight_copies(j):
        pairs = [
            (rel.at[j], rel.at[j]),
            (wk if j is c else wbuf.at[j, 1], wbuf.at[j, 1]),
            (wv if j is c else wbuf.at[j, 2], wbuf.at[j, 2]),
            (wq if j is c else wbuf.at[j, 0], wbuf.at[j, 0]),
            (wo if j is c else wout.at[j], wout.at[j]),
        ]
        return [
            remote(a, b, w_send.at[i], w_recv.at[i], sp, pair) for i, (a, b) in enumerate(pairs)
        ]

    weights, theirs = weight_copies(c), weight_copies(o)
    for cp in m1 + weights[:1] + lats[:2] + weights[1:]:
        cp.start()

    lane = lax.broadcasted_iota(jnp.int32, (W, 128), 1)
    col = lax.broadcasted_iota(jnp.int32, (W, 128), 0)
    key = lane % W
    start = jnp.clip(col - 8, 0, 48)
    inside = (key >= start) & (key < start + 16)

    def build(j, first, last):
        def one(h, carry):
            for a in range(14):
                r = jnp.broadcast_to(rel[j, a, pl.ds(h, 1), :] * LOG2E, (W, 128))
                r = pltpu.roll(r, 113, 1, stride=1, stride_axis=0)
                table[4 * j + h, a] = jnp.where(inside, r, MASKED)
            return carry

        lax.fori_loop(first, last, one, 0)

    build(c, 0, 4)

    for cp in m1:
        cp.wait_recv()
    modall[tp] = jnp.sum(modrecv[...], axis=0)
    m2 = [
        remote(modall.at[tp], modall.at[tp], m2_send.at[d], m2_recv.at[d], sp, (tp + d) % N_TP)
        for d in range(1, N_TP)
    ]
    for cp in m2 + lats[2:]:
        cp.start()
    theirs[0].wait_recv()
    build(o, 0, 2)
    local[3].wait()
    plain = ctx[...].astype(F32)
    normed[...] = plain * lax.rsqrt(jnp.mean(plain * plain, axis=-1, keepdims=True) + EPSILON)
    for d in range(1, N_TP):
        ref = modall.at[(tp + N_TP - d) % N_TP]
        remote(ref, ref, m2_send.at[d], m2_recv.at[d], sp, pair).wait_recv()

    def mod_row(i):
        return jnp.concatenate([modall[t, pl.ds(i, 1), :] for t in range(N_TP)], axis=1)

    g = gain[...].reshape(1, D)
    for s in range(2):
        gate[s : s + 1] = mod_row(6 + s)
    shift, scaled = mod_row(c), g * (1.0 + mod_row(3 + c))
    ctx_shift, ctx_scaled = mod_row(2), g * (1.0 + mod_row(5))

    for cp in local[4:8]:
        cp.wait()
    hid[0:64] = (normed[...] * ctx_scaled + ctx_shift).astype(BF16)
    for cp in theirs[1:4]:
        cp.wait_recv()
    first = []
    for j in range(2):
        for kind in range(2):
            ckv[j, kind, z, x] = jnp.dot(
                hid[0:64], wbuf[j, 1 + kind], preferred_element_type=F32
            ).astype(BF16)
        own = ckv.at[j, :, z, x]
        for d in (2, 1, 3):
            k = 3 * j + d - 1
            to = 4 * z + (x + d) % 4 if j == 0 else 4 * ((z + d) % 4) + x
            first.append(remote(own, own, ca_send.at[k], ca_recv.at[k], to, tp))
            first[-1].start()

    def unit(yy, k):
        for r in range(2):
            hid[64 * r : 64 * (r + 1)] = modulated(lat[2 * yy + r], scaled, shift)
        rows_q = pl.ds(pl.multiple_of(yy * 128, 128), 128)
        rows_k = pl.ds(pl.multiple_of(256 + yy * 128, 128), 128)
        hi = yy // 2
        to = pl.multiple_of(128 * (yy - 2 * hi) + 768 * (1 - hi), 128)
        cp = remote(
            kv.at[:, rows_k, :],
            kv.at[:, pl.ds(to, 128), :],
            h_send.at[k],
            h_recv.at[yy],
            (sp + 2 * hi - 1 + N_SP) % N_SP,
            tp,
        )
        to_sp = sp + 2 * hi - 1
        inner = (to_sp >= 0) & (to_sp < N_SP)
        for kind in (1, 2, 0):
            for j in range(2):
                cols = slice(256 * j, 256 * (j + 1))
                r = jnp.dot(hid[...], wbuf[j, kind], preferred_element_type=F32)
                if kind == 0:
                    q[rows_q, cols] = (r * (0.125 * LOG2E)).astype(BF16)
                else:
                    kv[kind - 1, rows_k, cols] = r.astype(BF16)
        return inner, cp

    def start_halo(halo):
        pl.when(halo[0])(halo[1].start)

    def arrived(ref, send, recv):
        remote(ref, ref, send, recv, sp, pair).wait_recv()

    def lat_wait(row, slot):
        arrived(lat.at[row], lat_send.at[slot], lat_recv.at[slot])

    lat_wait(2 * y + o, 0)
    halos = [unit(y, 0)]
    start_halo(halos[0])
    build(o, 2, 4)

    lat_wait(2 * down, 1)
    ref = lat.at[2 * down]
    lats.append(remote(ref, ref, lat_send.at[5], lat_recv.at[5], sp, 2 * up + c))
    lats[-1].start()
    lat_wait(2 * up + 1, 4)
    ref = lat.at[2 * up + 1]
    lats.append(remote(ref, ref, lat_send.at[6], lat_recv.at[6], sp, 2 * down + c))
    lats[-1].start()

    for d in range(1, 4):
        arrived(ckv.at[0, :, z, (x + 4 - d) % 4], ca_send.at[d - 1], ca_recv.at[d - 1])
        arrived(ckv.at[1, :, (z + 4 - d) % 4, x], ca_send.at[d + 2], ca_recv.at[d + 2])
    routes = [
        (4 * z_up + x, ckv.at[0, :, z, 0:2], ckv.at[0, :, z, 2:4]),
        (4 * z_down + x, ckv.at[0, :, z, 2:4], ckv.at[0, :, z, 0:2]),
        (4 * z + x_up, ckv.at[1, :, 0:2, x], ckv.at[1, :, 2:4, x]),
        (4 * z + x_down, ckv.at[1, :, 2:4, x], ckv.at[1, :, 0:2, x]),
    ]
    second = []
    for part_of in range(2):
        for i, (to, *halves) in enumerate(routes):
            ref, k = halves[part_of], 4 * part_of + i
            cp = remote(ref, ref, cb_send.at[k], cb_recv.at[k], to, tp)
            cp.start()
            second.append(cp)

    lat_wait(2 * down + 1, 2)
    halos.append(unit(down, 1))
    lat_wait(2 * up, 3)
    halos.append(unit(up, 2))

    z_opp, x_opp = (z + 2) % 4, (x + 2) % 4
    passed = [
        (ckv.at[0, :, z_down, 0:2], 4 * z_up + x),
        (ckv.at[0, :, z_up, 2:4], 4 * z_down + x),
        (ckv.at[1, :, 0:2, x_down], 4 * z + x_up),
        (ckv.at[1, :, 2:4, x_up], 4 * z + x_down),
    ]
    for i, (half, to) in enumerate(passed):
        arrived(half, cb_send.at[i], cb_recv.at[i])
        cp = remote(half, half, cb_send.at[8 + i], cb_recv.at[8 + i], to, tp)
        cp.start()
        second.append(cp)
    for halo in halos[1:]:
        start_halo(halo)

    lat_wait(2 * opp, 5)
    lat_wait(2 * opp + 1, 6)
    halos.append(unit(opp, 3))
    start_halo(halos[-1])

    rest = [
        ckv.at[0, :, z_down, 2:4],
        ckv.at[0, :, z_up, 0:2],
        ckv.at[1, :, 2:4, x_down],
        ckv.at[1, :, 0:2, x_up],
        ckv.at[0, :, z_opp, 0:2],
        ckv.at[0, :, z_opp, 2:4],
        ckv.at[1, :, 0:2, x_opp],
        ckv.at[1, :, 2:4, x_opp],
    ]
    for i in range(4):
        arrived(rest[i], cb_send.at[4 + i], cb_recv.at[4 + i])

    ones_near = jnp.ones((512, 128), BF16)
    left = lax.broadcasted_iota(jnp.int32, (512, 128), 1) < W

    def far(zs, xs, again):
        for hp in range(4):
            lanes = slice(128 * hp, 128 * (hp + 1))
            within = slice(128 * (hp % 2), 128 * (hp % 2 + 1))

            def tokens(kind):
                if hp < 2:
                    blocks = [ckv[0, kind, k, :, :, within].reshape(256, 128) for k in zs]
                else:
                    blocks = [ckv[1, kind, :, k, :, within].reshape(256, 128) for k in xs]
                return jnp.concatenate(blocks, axis=0)

            qp, kp = q[:, lanes], tokens(0)
            vp = jnp.concatenate([tokens(1), jnp.ones((256 * len(zs), 128), BF16)], axis=1)
            for half in range(2):
                h = 2 * hp + half
                qh = jnp.where(left if half == 0 else ~left, qp, jnp.zeros_like(qp))
                s = lax.dot_general(qh, kp, (((1,), (1,)), ((), ())), preferred_element_type=F32)
                m = jnp.max(s, axis=-1, keepdims=True)
                if not again:
                    p = jnp.exp2(s - m).astype(BF16)
                    far_o[h] = jnp.dot(p, vp, preferred_element_type=F32)
                    far_m[h] = jnp.broadcast_to(m, (512, 128))
                    continue
                m_old = far_m[h]
                m = jnp.maximum(m, m_old)
                alpha = jnp.exp2(m_old - m)
                p = jnp.exp2(s - jnp.concatenate([m] * 2, axis=1)).astype(BF16)
                o_new = jnp.dot(p, vp, preferred_element_type=F32)
                far_o[h, :, :128] = o_new[:, :128] + alpha * far_o[h, :, :128]
                far_o[h, :, 128:] = o_new[:, 128:] + alpha * far_o[h, :, 128:]
                far_m[h] = m + rel[h // 4, 15, h % 4 : h % 4 + 1, :] * LOG2E

    far((z, z_up, z_down), (x, x_up, x_down), False)
    for i in range(4, 8):
        arrived(rest[i], cb_send.at[4 + i], cb_recv.at[4 + i])
    far((z_opp,), (x_opp,), True)

    def halo_wait(yy):
        hi = yy // 2
        at = pl.ds(pl.multiple_of(128 * (yy - 2 * hi) + 768 * (1 - hi), 128), 128)
        of_sp = sp + 1 - 2 * hi

        @pl.when((of_sp >= 0) & (of_sp < N_SP))
        def _():
            arrived(kv.at[:, at, :], h_send.at[yy], h_recv.at[yy])

    for yy in (y, up, down):
        halo_wait(yy)
    theirs[4].wait_recv()
    local[8].wait()

    def near(yy):
        def one(r, carry):
            row = 2 * yy + r
            g = sp * 8 + row
            r0 = jnp.clip(g - 4, 0, 120)
            base = pl.multiple_of((r0 - sp * 8 + 4) * W, W)
            a0 = r0 - g + 7
            at = pl.ds(pl.multiple_of(row * W, W), W)
            for hp in range(4):
                lanes = slice(128 * hp, 128 * (hp + 1))
                qp = q[at, lanes]
                kp = kv[0, pl.ds(base, 512), lanes]
                vp = jnp.concatenate([kv[1, pl.ds(base, 512), lanes], ones_near], axis=1)
                zero = jnp.zeros_like(qp)
                qs = jnp.concatenate(
                    [jnp.where(lane < W, qp, zero), jnp.where(lane < W, zero, qp)], axis=0
                )
                s = lax.dot_general(qs, kp, (((1,), (1,)), ((), ())), preferred_element_type=F32)

                def of_pair(get):
                    return jnp.concatenate([get(2 * hp), get(2 * hp + 1)], axis=0)

                s = s + of_pair(
                    lambda h: jnp.concatenate([table[h, a0 + 2 * k] for k in range(4)], axis=1)
                )
                m1 = of_pair(lambda h: far_m[h, at, :])
                m = jnp.maximum(jnp.max(s, axis=-1, keepdims=True), m1)
                alpha = jnp.exp2(m1 - m)
                p = jnp.exp2(s - jnp.concatenate([m] * 4, axis=1)).astype(BF16)
                close = jnp.dot(p, vp, preferred_element_type=F32)
                top = close[:, :128] + alpha * of_pair(lambda h: far_o[h, at, :128])
                total = close[:, 128:] + alpha * of_pair(lambda h: far_o[h, at, 128:])
                both = top / total
                att[pl.ds(pl.multiple_of(r * W, W), W), lanes] = jnp.where(
                    lane < W, both[:W], both[W:]
                ).astype(BF16)
            return carry

        lax.fori_loop(0, 2, one, 0)
        full = wout[...].reshape(512, D)
        part[yy] = jnp.dot(att[...], full, preferred_element_type=F32).astype(BF16)

    def row(yy, r):
        return part.at[yy, pl.ds(pl.multiple_of(r * W, W), W), :]

    def send(k, src, slot, to):
        cp = remote(src, inbox.at[c, slot], i_send.at[k], i_recv.at[c, slot], sp, to)
        cp.start()
        return cp

    near(opp)
    relays = [
        remote(row(opp, 0), relay.at[0], r_send.at[0], r_recv.at[0], sp, 2 * up + c),
        remote(row(opp, 1), relay.at[1], r_send.at[1], r_recv.at[1], sp, 2 * down + c),
    ]
    for cp in relays:
        cp.start()
    e = y // 2
    second_y, third_y = (y + 1 + 2 * e) % 4, (y + 3 + 2 * e) % 4
    near(second_y)
    sends = [send(0, row(second_y, 1 - e), e, 2 * second_y + 1 - e)]
    halo_wait(opp)
    near(third_y)
    sends.append(send(1, row(third_y, e), 1 - e, 2 * third_y + e))
    near(y)
    sends.append(send(2, row(y, o), 2, pair))
    inbox[c, 2] = part[y, pl.ds(pl.multiple_of(c * W, W), W), :]
    for k, yy, r in ((3, second_y, e), (4, third_y, 1 - e)):
        arrived(relay.at[r], r_send.at[r], r_recv.at[r])
        mine_too = part[yy, pl.ds(pl.multiple_of(r * W, W), W), :]
        comb[r] = (mine_too.astype(F32) + relay[r].astype(F32)).astype(BF16)
        sends.append(send(k, comb.at[r], r, 2 * yy + r))

    def got(s, k):
        arrived(inbox.at[s, k], i_send.at[k], i_recv.at[s, k])

    local[9].wait()
    got(o, 2)
    for s in range(2):
        got(s, 0)
        got(s, 1)
    for s in range(2):
        update = inbox[s, 0].astype(F32) + inbox[s, 1].astype(F32) + inbox[s, 2].astype(F32)
        out[s] = (mine[s].astype(F32) + gate[s : s + 1] * update).astype(BF16)
    for cp in lats + weights + m1 + m2 + first + second + relays + sends:
        cp.wait_send()
    for inner, cp in halos:
        pl.when(inner)(cp.wait_send)


VM = pl.BlockSpec(memory_space=pltpu.VMEM)
SM = pl.BlockSpec(memory_space=pltpu.SMEM)
ANY = pl.BlockSpec(memory_space=pltpu.HBM)
DMA = pltpu.SemaphoreType.DMA


def on_device(*args):
    args = [*args[:12], args[12].transpose(1, 0, 2), args[13]]
    args = [pltpu.with_memory_space_constraint(a, pltpu.HBM) for a in args]
    return pl.pallas_call(
        kernel,
        out_shape=jax.ShapeDtypeStruct((2, W, D), BF16),
        in_specs=[ANY, ANY, VM, VM, ANY, ANY, ANY, VM, ANY, ANY, ANY, ANY, VM, SM],
        out_specs=VM,
        scratch_shapes=[
            pltpu.VMEM((512, 512), BF16),
            pltpu.VMEM((2, 1024, 512), BF16),
            pltpu.VMEM((2, 2, NZ, NX, 64, 256), BF16),
            pltpu.VMEM((2, 256, D), BF16),
            pltpu.VMEM((2, 16, 4, 128), F32),
            pltpu.VMEM((2, D), F32),
            pltpu.VMEM((8, W, D), BF16),
            pltpu.VMEM((W, D), BF16),
            pltpu.VMEM((3, 128, 256), BF16),
            pltpu.VMEM((2, 3, D, 256), BF16),
            pltpu.VMEM((8, 128), F32),
            pltpu.VMEM((1, D), F32),
            pltpu.VMEM((16, 8, 256), F32),
            pltpu.VMEM((8, 8, 256), F32),
            pltpu.VMEM((128, D), BF16),
            pltpu.VMEM((8, 14, W, 128), F32),
            pltpu.VMEM((8, 512, 256), F32),
            pltpu.VMEM((8, 512, 128), F32),
            pltpu.VMEM((128, 512), BF16),
            pltpu.VMEM((4, 128, D), BF16),
            pltpu.VMEM((2, W, D), BF16),
            pltpu.VMEM((2, W, D), BF16),
            pltpu.VMEM((2, 3, W, D), BF16),
            pltpu.VMEM((2, W, D), BF16),
            pltpu.VMEM((W, D), F32),
            DMA((10,)),
            DMA((5,)), DMA((5,)), DMA((7,)), DMA((7,)),
            DMA((16,)), DMA((16,)), DMA((8,)), DMA((8,)),
            DMA((6,)), DMA((6,)), DMA((12,)), DMA((12,)), DMA((4,)), DMA((4,)),
            DMA((2,)), DMA((2,)), DMA((5,)), DMA((2, 3)),
        ],
        compiler_params=pltpu.CompilerParams(
            collective_id=0, has_side_effects=True, vmem_limit_bytes=48 * 2**20
        ),
        name="layer",
    )(*args)


def solution(mesh):
    return jax.shard_map(
        on_device,
        mesh=mesh,
        in_specs=(
            P(None, ("sp", "tp"), None),
            P(None, "sp", None),
            P(),
            P(),
            P("sp", "tp"),
            P("sp", "tp"),
            P("sp", "tp"),
            P(),
            P(None, "tp"),
            P(None, "tp"),
            P(None, "tp"),
            P("tp", None),
            P("tp", None, None),
            P("tp"),
        ),
        out_specs=P(None, ("sp", "tp"), None),
        check_vma=False,
    )
```
